32 devices in a mesh: gr: 2 (over x), fs: 4 (over z), tp: 4 (over y, core).
Axes of the slice: x: 2, y: 2, z: 4, core: 2. Of those that a mesh axis runs over, the one named last changes fastest.
Arguments:
- tokens: bfloat16 [4096, 2048], P(('gr', 'fs')), may hold values from -6 to 6
- routes: int32 [4096, 2], P(('gr', 'fs')), may hold values from 0 to 3, all different within a row; in each aligned block of 512 rows (0 to 511, 512 to 1023, ...) at most 384 rows name the same one
- route_weight: float32 [4096, 2], P(('gr', 'fs')), may hold values from 0.2 to 1
- gain: float32 [2048], P(('gr', 'fs')), may hold values from 0.1 to 1.9
- w_gate: bfloat16 [4, 2048, 4096], P(None, ('gr', 'fs'), 'tp'), may hold values from -0.125 to 0.125
- w_up: bfloat16 [4, 2048, 4096], P(None, ('gr', 'fs'), 'tp'), may hold values from -0.125 to 0.125
- w_down: bfloat16 [4, 2048, 4096], P(None, ('gr', 'fs'), 'tp'), may hold values from -0.09375 to 0.09375
Outputs:
- gate_out: bfloat16 [4, 2048, 4096], P('fs', None, 'tp')
- up_out: bfloat16 [4, 2048, 4096], P('fs', None, 'tp')
- down_out: bfloat16 [4, 2048, 4096], P('fs', None, 'tp')
- mixed: bfloat16 [4096, 2048], P(('gr', 'fs'), 'tp')
The draws below stay inside these ranges and needn't reach their ends.
Inputs may be any that keep to these rules, and one draw needn't show every extreme that they name: `routes`: each row names two different experts. Among the 512 rows of one device no expert is named more than 384 times, and in every draw some device names some expert exactly 384 times.
All inputs are finite; a program needn't handle non-finite values.
Results may differ from the reference program's by a relative error of at most 0.015.
Values may be sent and summed in bfloat16 or wider, within the bound.
A program may use at most 128 MiB of HBM per device.

```python
import math
import jax
import jax.numpy as jnp
import numpy as np
from jax import lax

D = 2048
FF = 4096
EXPERTS = 4
TOK_DEV = 512
CAP = 384
TOKENS = 4096
N_GR = 2
N_FS = 4
N_TP = 4


def level_of(rng, extent, cuts, low, largest):
    def one(position, shards_of):
        heights = jax.random.uniform(jax.random.fold_in(jax.random.fold_in(rng, 6), position), (shards_of,), jnp.float32, low / len(cuts), largest / len(cuts))
        return jnp.repeat(jnp.exp(heights), extent[position] // shards_of).reshape((-1,) + (1,) * (len(extent) - position - 1))

    factor_of = one(*cuts[0])
    for cut in cuts[1:]:
        factor_of = factor_of * one(*cut)
    return factor_of


def deal_out(own_key, own, number, rows, amount, top, bound, skew):
    order = jax.random.permutation(own_key, amount)
    heavy_load, ordinary = portions_of(amount, rows * top, bound, skew, True), portions_of(amount, rows * top, bound, skew, False)
    places = jnp.arange(amount)

    def named(tallies, rotation):
        used = int((tallies > 0).sum())
        fixed = max(1, used // 4)
        passed = fixed + (places - fixed + rotation * (used - fixed)) % max(1, amount - fixed)
        return jnp.zeros((amount,), jnp.int32).at[order[jnp.where(places < fixed, places, passed)]].set(jnp.asarray(tallies, jnp.int32))

    tallies = jnp.where(number % 4 == 0, named(heavy_load, number // 4), named(ordinary, number - number // 4 - 1))
    mixed = jax.random.permutation(jax.random.fold_in(own, 3), amount)
    donor, sink = mixed[0:amount // 2 * 2:2], mixed[1:amount // 2 * 2:2]
    margin = jnp.minimum(tallies[donor] - 1, bound - tallies[sink]) // 2
    margin = jnp.where((donor == order[0]) | (sink == order[0]) | (tallies[sink] == 0), 0, jnp.maximum(margin, 0))
    passed = jax.random.randint(jax.random.fold_in(own, 4), (amount // 2,), 0, 1 << 20) % (margin + 1)
    tallies = tallies.at[donor].add(-passed).at[sink].add(passed)
    members = jnp.searchsorted(jnp.cumsum(tallies), jnp.arange(rows * top), side="right").astype(jnp.int32)
    table = members.reshape(top, rows).T
    table = table[jax.random.permutation(jax.random.fold_in(own, 1), rows)]
    rotation = jax.random.randint(jax.random.fold_in(own, 2), (rows, 1), 0, top)
    return jnp.take_along_axis(table, (jnp.arange(top)[None, :] + rotation) % top, axis=1)


def portions_of(number_of, total, most, slope, full):
    portions = [(1 << 20) // math.isqrt(standing ** slope) + 1 for standing in range(1, number_of + 1)]
    largest = most if full else min(most, max(-(-total // number_of), total * portions[0] // sum(portions)))
    least = 1 if total - largest >= number_of - 1 else 0
    counts, spare = [largest] + [least] * (number_of - 1), total - largest - least * (number_of - 1)
    while spare > 0:
        candidates = [i for i in range(1, number_of) if counts[i] < largest] or [i for i in range(1, number_of) if counts[i] < most]
        pool, budget = sum([portions[i] for i in candidates]), spare
        for i in candidates:
            extra = min(most - counts[i], max(1, budget * portions[i] // pool), spare)
            counts[i] = counts[i] + extra
            spare = spare - extra
    return np.array(counts)


def gaussian(stream_key, shape, scale, most, shards=(), kind=jnp.bfloat16):
    level = level_of(stream_key, shape, shards, -0.22, 0.18) if shards else 1.0
    drawn = jax.random.normal(stream_key, shape, jnp.float32) * scale * level
    return jnp.minimum(jnp.maximum(drawn, -most), most).astype(kind)


def setup_inputs(seed: int = 0) -> dict:
    keys = jax.random.split(jax.random.key(seed), 8)
    tokens = gaussian(keys[0], (TOKENS, D), 1.0, 6.0, ((0, 8),))
    routes_keys = jax.random.split(jax.random.fold_in(keys[1], 1), TOKENS // TOK_DEV)
    routes_turns = jax.random.permutation(jax.random.fold_in(keys[1], 3), TOKENS // TOK_DEV)
    routes = jax.vmap(lambda own, number: deal_out(jax.random.fold_in(keys[1], 2), own, number, TOK_DEV, EXPERTS, 2, CAP, 2))(routes_keys, routes_turns).reshape((TOKENS, 2))
    route_weight = jnp.clip(jnp.exp(math.log(1.0) - 1.609438 * jax.random.uniform(keys[2], (TOKENS, 2), jnp.float32) ** level_of(keys[2], (TOKENS, 2), ((0, 8),), -0.2, 0.2)), 0.2, 1.0)
    gain = jnp.clip(1.0 + 0.18 * jax.random.normal(keys[3], (D,), jnp.float32), 0.1, 1.9)
    w_gate = gaussian(keys[4], (EXPERTS, D, FF), D ** -0.5, 0.125, ((1, 8), (2, 4)))
    w_up = gaussian(keys[5], (EXPERTS, D, FF), D ** -0.5, 0.125, ((1, 8), (2, 4)))
    w_down = gaussian(keys[6], (EXPERTS, D, FF), FF ** -0.5, 0.09375, ((1, 8), (2, 4)))
    return dict(tokens=tokens, routes=routes, route_weight=route_weight, gain=gain, w_gate=w_gate, w_up=w_up, w_down=w_down)


EPSILON = 1e-05

def expert_rows(pieces):
    rows, gate_w, up_w, down_w = pieces
    gate = jnp.dot(rows, gate_w, preferred_element_type=jnp.float32)
    upper = jnp.dot(rows, up_w, preferred_element_type=jnp.float32)
    hidden = (jax.nn.silu(gate) * upper).astype(jnp.bfloat16)
    count = rows.shape[0]
    blocked = hidden.reshape(count, N_TP, FF // N_TP).astype(jnp.float32)
    down_blocks = down_w.reshape(D, N_TP, FF // N_TP).astype(jnp.float32)
    partial_value = jnp.einsum('rjf,djf->jrd', blocked, down_blocks)
    rounded = lax.optimization_barrier(partial_value.astype(jnp.bfloat16))
    return lax.optimization_barrier(jnp.sum(rounded.astype(jnp.float32), axis=0)).astype(jnp.bfloat16)

def reference(tokens, routes, route_weight, gain, w_gate, w_up, w_down):
    scaling = gain[None, :, None]
    gate_out = (w_gate.astype(jnp.float32) * scaling).astype(jnp.bfloat16)
    up_out = (w_up.astype(jnp.float32) * scaling).astype(jnp.bfloat16)
    down_out = w_down
    float_rows = tokens.astype(jnp.float32)
    normed = (float_rows * lax.rsqrt(lax.optimization_barrier(jnp.mean(float_rows * float_rows, axis=-1, keepdims=True)) + EPSILON)).astype(jnp.bfloat16)
    groups = N_GR * N_FS
    flat_ids = routes.reshape(groups, TOK_DEV * 2)
    onehot = (flat_ids[:, :, None] == jnp.arange(EXPERTS, dtype=jnp.int32)[None, None, :]).astype(jnp.int32)
    slot_rank = lax.optimization_barrier(jnp.sum((jnp.cumsum(onehot, axis=1) - onehot) * onehot, axis=-1))
    group_ids = jnp.arange(groups, dtype=jnp.int32)[:, None]
    destination = (flat_ids * (groups * CAP) + group_ids * CAP + slot_rank).reshape(-1).astype(jnp.int32)
    token_ids = (jnp.arange(TOKENS * 2, dtype=jnp.int32) // 2).astype(jnp.int32)
    source = jnp.zeros((EXPERTS * groups * CAP,), jnp.int32).at[destination].set(token_ids)
    gathered = normed[source].reshape(EXPERTS, groups * CAP, D)
    outputs = lax.map(expert_rows, (gathered, gate_out, up_out, down_out))
    flat_out = outputs.reshape(EXPERTS * groups * CAP, D)
    picked = flat_out[destination].reshape(TOKENS, 2, D).astype(jnp.float32)
    mixed = lax.optimization_barrier(jnp.sum(route_weight[:, :, None] * picked, axis=1)).astype(jnp.bfloat16)
    return (gate_out, up_out, down_out, mixed)
```

```python
import functools
import jax
import jax.numpy as jnp
from jax import lax
from jax.experimental import pallas as pl
from jax.experimental.pallas import tpu as pltpu
from jax.sharding import PartitionSpec as P

MESH = pl.DeviceIdType.MESH
VMEM_LIMIT = 50 * 1024 * 1024
EPSILON = 1e-05
BLOCKS = 4
LAG = 4


def kernel(ng, nz, nt, tok_in, routes, rweight, gain, gw, uw, dw, gout, uout, dout, mixed,
           tok, hid, part, crx, yrx, stage, raw, ret, rly, wsend, wrecv, wcol, gcol,
           ld, ts, tr, fs_s, fr, gs, gr, zs, zr, xs, xr, cs, cr, ys, yr, hs, hr, rs, rr):
    g, z, t = lax.axis_index("gr"), lax.axis_index("fs"), lax.axis_index("tp")
    core, y = lax.rem(t, 2), lax.div(t, 2)
    rows, d = tok_in.shape
    quarter = d // nt
    chunk, width = gw.shape[1], gw.shape[2]
    half = chunk // 2
    chunks = ng * nz
    per_owner = chunks // nt
    nb = BLOCKS
    blk = width // nb
    outs = (gout, uout)
    mate, over = y * 2 + 1 - core, (1 - y) * 2 + core
    inner = jnp.logical_and(z > 0, z < nz - 1)
    side = lax.div(z, 2)
    pair = z + 1 - 2 * lax.rem(z, 2)
    far = (3 * (1 - side), 2 - side)
    order = (far[0], far[1], pair, z)

    def to(k):
        return lax.rem(z + k, nz)

    def frm(k):
        return lax.rem(z + nz - k, nz)

    def rdma(src, dst, ss, rsem, dev):
        return pltpu.make_async_remote_copy(
            src_ref=src, dst_ref=dst, send_sem=ss, recv_sem=rsem, device_id=dev, device_id_type=MESH
        )

    def row0(group, zsrc):
        return pl.multiple_of((group * nz + zsrc) * chunk, chunk)

    def cols(b):
        return pl.ds(pl.multiple_of(b * blk, blk), blk)

    def qcols(q):
        return pl.ds(pl.multiple_of(q * quarter, quarter), quarter)

    def piece(m, b, group, zsrc):
        return outs[m].at[pl.ds(row0(group, zsrc), chunk), cols(b)]

    def dpiece(m, group, zsrc):
        return dout.at[pl.ds(pl.multiple_of(row0(group, zsrc) + m * half, half), half), :]

    def z_copy(m, b, k):
        return rdma(stage.at[m, to(k), :, cols(b)], piece(m, b, g, z), zs.at[m, b, k], zr.at[m, b, k], {"fs": to(k)})

    def zd_copy(m, k):
        return rdma(dw.at[to(k), pl.ds(m * half, half), :], dpiece(m, g, z), zs.at[m, nb, k], zr.at[m, nb, k], {"fs": to(k)})

    def x_own(m, b):
        return rdma(stage.at[m, z, :, cols(b)], piece(m, b, g, z), xs.at[m, b, 0], xr.at[m, b, 0], {"gr": 1 - g})

    def xd_own(m):
        return rdma(dw.at[z, pl.ds(m * half, half), :], dpiece(m, g, z), xs.at[m, nb, 0], xr.at[m, nb, 0], {"gr": 1 - g})

    def relay(ref, m, b, k):
        return rdma(ref, ref, xs.at[m, b, k], xr.at[m, b, k], {"gr": 1 - g})

    def z_arrive(ref, m, b, k):
        rdma(ref, ref, zs.at[m, b, k], zr.at[m, b, k], {"fs": to(k)}).wait_recv()

    def z_take(b, k):
        for m in range(2):
            ref = piece(m, b, g, frm(k))
            z_arrive(ref, m, b, k)
            relay(ref, m, b, k).start()

    def zd_take(k):
        for m in range(2):
            ref = dpiece(m, g, frm(k))
            z_arrive(ref, m, nb, k)
            relay(ref, m, nb, k).start()

    def z_block(b):
        for k in range(1, nz):
            for m in range(2):
                z_copy(m, b, k).start()

    def z_down():
        for k in range(1, nz):
            for m in range(2):
                zd_copy(m, k).start()

    load_tok = pltpu.make_async_copy(tok_in, raw, ld.at[0])
    loads = [pltpu.make_async_copy(src, stage.at[m], ld.at[1 + m]) for m, src in enumerate((gw, uw))]
    own_rows = pl.ds(row0(g, z), chunk)
    own_down = pltpu.make_async_copy(dw.at[z], dout.at[own_rows, :], ld.at[3])
    load_tok.start()
    for c in loads:
        c.start()
    own_down.start()

    barrier = pltpu.get_barrier_semaphore()
    for k in range(1, nz):
        pl.semaphore_signal(barrier, inc=1, device_id={"fs": to(k)}, device_id_type=MESH)
    for who in (mate, over):
        pl.semaphore_signal(barrier, inc=1, device_id={"tp": who}, device_id_type=MESH)
    pl.semaphore_signal(barrier, inc=1, device_id={"gr": 1 - g}, device_id_type=MESH)

    step = 64
    load_tok.wait()

    @pl.loop(0, rows // step)
    def _(i):
        at = pl.ds(pl.multiple_of(i * step, step), step)
        v = raw[at, :].astype(jnp.float32)
        scale = lax.rsqrt(jnp.mean(v * v, axis=-1, keepdims=True) + EPSILON)
        tok[z, at, :] = (v * scale).astype(jnp.bfloat16)

    pl.semaphore_wait(barrier, nz - 1 + 3)

    guarded = []

    def guard(flag, c):
        @pl.when(flag)
        def _():
            c.start()
        guarded.append((flag, c))

    def hop(way, h, src):
        ref = tok.at[src, :, qcols(t)]
        nxt = lax.rem(z + way + nz, nz)
        return rdma(ref, ref, ts.at[(way + 1) // 2, h], tr.at[src], {"fs": nxt})

    right, left = z + 1 < nz, z >= 1
    guard(right, hop(1, 0, z))
    guard(left, hop(-1, 0, z))
    for m in range(2):
        xd_own(m).start()

    gcol[...] = jnp.transpose(jnp.broadcast_to(gain[...], (128, chunk)))
    for c in loads:
        c.wait()

    @pl.loop(0, nz * (chunk // step))
    def _(i):
        e = i // (chunk // step)
        at = pl.ds(pl.multiple_of(lax.rem(i, chunk // step) * step, step), step)
        factor = jnp.concatenate([gcol[at, :]] * (width // 128), axis=1)
        for m in range(2):
            stage[m, e, at, :] = (stage[m, e, at, :].astype(jnp.float32) * factor).astype(jnp.bfloat16)

    z_block(0)

    @pl.when(jnp.logical_not(inner))
    def _():
        @pl.loop(1, nb)
        def _(b):
            z_block(b)
        z_down()

    for b in range(min(2, nb)):
        for m in range(2):
            x_own(m, b).start()

    for e in range(nz):
        wsend[e] = (
            jnp.where(routes[0:1, :] == e, rweight[0:1, :], 0.0)
            + jnp.where(routes[1:2, :] == e, rweight[1:2, :], 0.0)
        )
    wrecv[z] = wsend[z]
    for k in range(1, nz):
        rdma(wsend.at[to(k)], wrecv.at[z], gs.at[k], gr.at[k], {"fs": to(k)}).start()
    for m in range(2):
        outs[m][own_rows, :] = stage[m, z]

    for h in range(1, nz):
        for way in (1, -1):
            src = lax.rem(z - way * h + nz, nz)
            valid = z >= h if way == 1 else z + h < nz
            more = right if way == 1 else left
            ref = tok.at[src, :, qcols(t)]

            @pl.when(valid)
            def _(ref=ref, src=src):
                rdma(ref, ref, ts.at[0, 0], tr.at[src], {"fs": lax.rem(z + 1, nz)}).wait_recv()
            guard(jnp.logical_and(valid, more), hop(way, h, src))
            guard(valid, rdma(ref, ref, fs_s.at[1, src], fr.at[1, src], {"tp": over}))
            guard(valid, rdma(ref, ref, fs_s.at[0, src], fr.at[0, src], {"tp": mate}))
        if h == 1:
            @pl.when(inner)
            def _():
                z_block(1)
            z_take(0, 1)
        if h == 2:
            @pl.when(inner)
            def _():
                @pl.loop(2, nb)
                def _(b):
                    z_block(b)
            for k in range(2, nz):
                z_take(0, k)
            for b in range(2, nb):
                for m in range(2):
                    x_own(m, b).start()

    def token_quarter(lane, src, q):
        ref = tok.at[src, :, qcols(q)]
        return rdma(ref, ref, fs_s.at[lane, src], fr.at[lane, src], {"tp": mate})

    @pl.loop(nz, (nb + 1) * nz)
    def _(i):
        b, s = i // nz, lax.rem(i, nz)
        src = frm(s)
        k = s + 1
        take = s < nz - 1

        @pl.when(jnp.logical_and(take, b < nb))
        def _():
            z_take(b, k)

        @pl.when(jnp.logical_and(take, b == nb))
        def _():
            zd_take(k)

        @pl.when(jnp.logical_and(inner, i == nb * nz - 2))
        def _():
            z_down()

        @pl.when(s == 0)
        def _():
            @pl.loop(0, nz)
            def _(kk):
                for m in range(2):
                    ref = piece(m, b - 1, 1 - g, frm(kk))
                    rdma(ref, ref, xs.at[m, b - 1, kk], xr.at[m, b - 1, kk], {"gr": 1 - g}).wait_recv()

        @pl.when(b == 1)
        def _():
            @pl.when(s >= 1)
            def _():
                token_quarter(1, src, over).wait_recv()
                token_quarter(2, src, over).start()
                token_quarter(0, src, mate).wait_recv()
                token_quarter(2, src, (1 - y) * 2 + 1 - core).wait_recv()
                rdma(wrecv.at[src], wrecv.at[src], gs.at[s], gr.at[s], {"fs": to(s)}).wait_recv()
            wcol[src] = jnp.transpose(jnp.broadcast_to(wrecv[src], (128, rows)))

        a = tok[src]
        gate = jnp.dot(a, gout[:, cols(b - 1)], preferred_element_type=jnp.float32)
        upper = jnp.dot(a, uout[:, cols(b - 1)], preferred_element_type=jnp.float32)
        weight = jnp.concatenate([wcol[src]] * (blk // 128), axis=1)
        hid[src, :, cols(b - 1)] = (gate / (1.0 + jnp.exp(-gate)) * upper * weight).astype(jnp.bfloat16)

    own_down.wait()

    def chunk_of(i):
        k, other = i // 2, lax.rem(i, 2)
        group = g + other * (1 - 2 * g)
        c = group * nz + frm(k)
        owner = c // per_owner
        return k, other, c, owner, lax.rem(owner, 2), owner // 2, lax.rem(c, per_owner)

    def give(i):
        k, other, c, owner, par, yo, cc = chunk_of(i)
        return rdma(part.at[c], crx.at[yo * per_owner + cc], cs.at[i], cr.at[i], {"tp": mate})

    def up(i, j):
        k, other, c, owner, par, yo, cc = chunk_of(i)
        return rdma(part.at[c, order[j]], yrx.at[cc, order[j]], ys.at[i, j], yr.at[i, j], {"tp": over})

    def near(c, cc, j):
        dst = rly.at[j, cc] if j < 2 else ret.at[0, cc]
        return rdma(part.at[c, order[j]], dst, hs.at[j, cc], hr.at[j, cc], {"fs": pair})

    def cross(cc, j):
        return rdma(part.at[t * per_owner + cc, order[j]], ret.at[1, cc], rs.at[j, cc], rr.at[cc], {"fs": order[j]})

    def stage_a(i):
        k, other, c, owner, par, yo, cc = chunk_of(i)

        @pl.when(other == 1)
        def _():
            for m in range(2):
                ref = dpiece(m, 1 - g, frm(k))
                rdma(ref, ref, xs.at[m, nb, k], xr.at[m, nb, k], {"gr": 1 - g}).wait_recv()

        mine = pl.ds(pl.multiple_of(c * chunk, chunk), chunk)

        @pl.loop(0, nz)
        def _(b):
            part[c, b] = lax.dot_general(
                hid[b], dout[mine, :], (((1,), (1,)), ((), ())), preferred_element_type=jnp.float32
            ).astype(jnp.bfloat16)

        @pl.when(par != core)
        def _():
            give(i).start()

    def stage_b(i):
        k, other, c, owner, par, yo, cc = chunk_of(i)

        @pl.when(par == core)
        def _():
            slot = crx.at[yo * per_owner + cc]
            rdma(slot, slot, cs.at[i], cr.at[i], {"tp": mate}).wait_recv()
            for j in range(nz):
                b = order[j]
                part[c, b] = (
                    part[c, b].astype(jnp.float32) + crx[yo * per_owner + cc, b].astype(jnp.float32)
                ).astype(jnp.bfloat16)

                @pl.when(yo != y)
                def _(j=j):
                    up(i, j).start()

    def stage_c(i):
        k, other, c, owner, par, yo, cc = chunk_of(i)

        @pl.when(owner == t)
        def _():
            for j in range(nz):
                b = order[j]
                slot = yrx.at[cc, b]
                rdma(slot, slot, ys.at[i, j], yr.at[i, j], {"tp": over}).wait_recv()
                part[c, b] = (
                    part[c, b].astype(jnp.float32) + yrx[cc, b].astype(jnp.float32)
                ).astype(jnp.bfloat16)
                if j < 2:
                    @pl.when(jnp.logical_not(inner))
                    def _(j=j):
                        near(c, cc, j).start()
                elif j == 2:
                    near(c, cc, j).start()

    n = chunks

    @pl.loop(0, n + LAG)
    def _(i):
        @pl.when(i < n)
        def _():
            stage_a(i)

        @pl.when(jnp.logical_and(i >= 1, i - 1 < n))
        def _():
            stage_b(i - 1)

        @pl.when(i >= LAG)
        def _():
            stage_c(i - LAG)

    @pl.when(inner)
    def _():
        first = jnp.where(side == core, 0, 1)
        for turn in range(per_owner):
            cc = first + turn * (1 - 2 * first)
            for j in range(2):
                slot = rly.at[j, cc]
                rdma(slot, slot, hs.at[j, cc], hr.at[j, cc], {"fs": pair}).wait_recv()
                c, b = t * per_owner + cc, order[j]
                part[c, b] = (
                    part[c, b].astype(jnp.float32) + rly[j, cc].astype(jnp.float32)
                ).astype(jnp.bfloat16)
                cross(cc, j).start()

    for cc in range(per_owner):
        direct, crossed = ret.at[0, cc], ret.at[1, cc]
        rdma(direct, direct, hs.at[2, cc], hr.at[2, cc], {"fs": pair}).wait_recv()
        rdma(crossed, crossed, rs.at[0, cc], rr.at[cc], {"fs": pair}).wait_recv()
        mixed[:, cc * chunk:(cc + 1) * chunk] = (
            part[t * per_owner + cc, z].astype(jnp.float32)
            + ret[0, cc].astype(jnp.float32)
            + ret[1, cc].astype(jnp.float32)
        ).astype(jnp.bfloat16)

    @pl.loop(1, nz)
    def _(k):
        rdma(wsend.at[to(k)], wrecv.at[z], gs.at[k], gr.at[k], {"fs": to(k)}).wait_send()
        for m in range(2):
            zd_copy(m, k).wait_send()
            relay(dpiece(m, g, frm(k)), m, nb, k).wait_send()
        token_quarter(2, frm(k), over).wait_send()

        @pl.loop(0, nb)
        def _(b):
            for m in range(2):
                z_copy(m, b, k).wait_send()
                relay(piece(m, b, g, frm(k)), m, b, k).wait_send()

    for m in range(2):
        xd_own(m).wait_send()

        @pl.loop(0, nb)
        def _(b):
            x_own(m, b).wait_send()

    for flag, c in guarded:
        @pl.when(flag)
        def _(c=c):
            c.wait_send()

    @pl.loop(0, n)
    def _(i):
        k, other, c, owner, par, yo, cc = chunk_of(i)

        @pl.when(par != core)
        def _():
            give(i).wait_send()

        @pl.when(jnp.logical_and(par == core, yo != y))
        def _():
            for j in range(nz):
                up(i, j).wait_send()

    for cc in range(per_owner):
        c = t * per_owner + cc
        near(c, cc, 2).wait_send()
        for j in range(2):
            @pl.when(inner)
            def _(j=j, cc=cc):
                cross(cc, j).wait_send()

            @pl.when(jnp.logical_not(inner))
            def _(j=j, c=c, cc=cc):
                near(c, cc, j).wait_send()


def store(gate, upper, down, mixed, gate_out, up_out, down_out, mixed_out, sem):
    copies = [
        pltpu.make_async_copy(gate, gate_out.at[0], sem.at[0]),
        pltpu.make_async_copy(upper, up_out.at[0], sem.at[1]),
        pltpu.make_async_copy(down, down_out.at[0], sem.at[2]),
        pltpu.make_async_copy(mixed, mixed_out, sem.at[3]),
    ]
    for c in copies:
        c.start()
    for c in copies:
        c.wait()


def fused(ng, nz, nt, tokens, routes, route_weight, gain, w_gate, w_up, w_down):
    rows, d = tokens.shape
    quarter = d // nt
    experts, chunk, width = w_gate.shape
    chunks = ng * nz
    per_owner = chunks // nt
    bf, f32 = jnp.bfloat16, jnp.float32
    dma = pltpu.SemaphoreType.DMA
    full = pltpu.VMEM((d, width), bf)
    vmem = pl.BlockSpec(memory_space=pltpu.VMEM)
    anywhere = pl.BlockSpec(memory_space=pl.ANY)
    results = pl.pallas_call(
        functools.partial(kernel, ng, nz, nt),
        out_shape=(full, full, full, pltpu.VMEM((rows, quarter), bf)),
        in_specs=[anywhere, vmem, vmem, vmem, anywhere, anywhere, anywhere],
        out_specs=(vmem,) * 4,
        scratch_shapes=[
            pltpu.VMEM((nz, rows, d), bf),
            pltpu.VMEM((nz, rows, width), bf),
            pltpu.VMEM((chunks, nz, rows, chunk), bf),
            pltpu.VMEM((chunks // 2, nz, rows, chunk), bf),
            pltpu.VMEM((per_owner, nz, rows, chunk), bf),
            pltpu.VMEM((2, nz, chunk, width), bf),
            pltpu.VMEM((rows, d), bf),
            pltpu.VMEM((2, per_owner, rows, chunk), bf),
            pltpu.VMEM((2, per_owner, rows, chunk), bf),
            pltpu.VMEM((nz, 1, rows), f32),
            pltpu.VMEM((nz, 1, rows), f32),
            pltpu.VMEM((nz, rows, 128), f32),
            pltpu.VMEM((chunk, 128), f32),
            dma((4,)),
            dma((2, nz)), dma((nz,)),
            dma((3, nz)), dma((3, nz)),
            dma((nz,)), dma((nz,)),
            dma((2, BLOCKS + 1, nz)), dma((2, BLOCKS + 1, nz)),
            dma((2, BLOCKS + 1, nz)), dma((2, BLOCKS + 1, nz)),
            dma((chunks,)), dma((chunks,)),
            dma((chunks, nz)), dma((chunks, nz)),
            dma((3, per_owner)), dma((3, per_owner)),
            dma((2, per_owner)), dma((per_owner,)),
        ],
        compiler_params=pltpu.CompilerParams(
            collective_id=0, has_side_effects=True, vmem_limit_bytes=VMEM_LIMIT
        ),
    )(tokens, routes.T, route_weight.T, gain.reshape(1, chunk), w_gate, w_up, w_down)
    whole = jax.ShapeDtypeStruct((1, d, width), bf)
    return pl.pallas_call(
        store,
        out_shape=(whole, whole, whole, jax.ShapeDtypeStruct((rows, quarter), bf)),
        in_specs=[vmem] * 4,
        out_specs=(anywhere,) * 4,
        scratch_shapes=[dma((4,))],
        compiler_params=pltpu.CompilerParams(vmem_limit_bytes=4 * 1024 * 1024),
    )(*results)

EXP_DEV = 1


def body(tokens, routes, route_weight, gain, w_gate, w_up, w_down):
    scaling = gain[None, :, None]
    gate_local = (w_gate * scaling).astype(jnp.bfloat16)
    up_local = (w_up * scaling).astype(jnp.bfloat16)
    gate_mine, up_mine, down_mine = (
        lax.all_to_all(gate_local, "fs", split_axis=0, concat_axis=1, tiled=True),
        lax.all_to_all(up_local, "fs", split_axis=0, concat_axis=1, tiled=True),
        lax.all_to_all(w_down, "fs", split_axis=0, concat_axis=1, tiled=True),
    )
    gate_out, up_out, down_out = (
        lax.all_gather(gate_mine, "gr", axis=1, tiled=True),
        lax.all_gather(up_mine, "gr", axis=1, tiled=True),
        lax.all_gather(down_mine, "gr", axis=1, tiled=True),
    )
    fs_count = lax.axis_size("fs")
    experts = EXP_DEV * fs_count
    tok_rows = tokens.shape[0]
    capacity = 3 * tok_rows // experts
    float_rows = tokens.astype(jnp.float32)
    normed = (
        float_rows * lax.rsqrt(jnp.mean(float_rows * float_rows, axis=-1, keepdims=True) + EPSILON)
    ).astype(jnp.bfloat16)
    flat_ids = routes.reshape(-1)
    onehot = (flat_ids[:, None] == jnp.arange(experts, dtype=jnp.int32)[None, :]).astype(jnp.int32)
    slot_rank = jnp.sum((jnp.cumsum(onehot, axis=0) - onehot) * onehot, axis=-1)
    destination = (flat_ids * capacity + slot_rank).reshape(tok_rows, 2)
    slot_ids = jnp.arange(experts * capacity, dtype=jnp.int32)
    hits = slot_ids[:, None, None] == destination[None, :, :]
    dispatch = jnp.any(hits, axis=-1).astype(jnp.bfloat16)
    outgoing = jnp.dot(dispatch, normed, preferred_element_type=jnp.float32).astype(jnp.bfloat16)
    outgoing = outgoing.reshape(fs_count, EXP_DEV, capacity, tokens.shape[1])
    arrived = lax.all_to_all(outgoing, "fs", split_axis=0, concat_axis=0, tiled=True)
    gate = jnp.einsum("sjnd,jdf->sjnf", arrived, gate_out, preferred_element_type=jnp.float32)
    upper = jnp.einsum("sjnd,jdf->sjnf", arrived, up_out, preferred_element_type=jnp.float32)
    hidden = (jax.nn.silu(gate) * upper).astype(jnp.bfloat16)
    partial_value = jnp.einsum(
        "sjnf,jdf->sjnd", hidden, down_out, preferred_element_type=jnp.float32
    )
    rounded = lax.optimization_barrier(partial_value.astype(jnp.bfloat16))
    summed = lax.psum_scatter(
        rounded.astype(jnp.float32).astype(jnp.bfloat16), "tp", scatter_dimension=3, tiled=True
    )
    back_home = lax.all_to_all(summed, "fs", split_axis=0, concat_axis=0, tiled=True)
    features = back_home.shape[-1]
    flat_back = back_home.reshape(experts * capacity, features).astype(jnp.float32)
    first = jnp.where(slot_ids[None, :] == destination[:, 0:1], route_weight[:, 0:1], 0.0)
    second = jnp.where(slot_ids[None, :] == destination[:, 1:2], route_weight[:, 1:2], 0.0)
    combine_map = first + second
    mixed = jnp.dot(
        combine_map, flat_back, precision=lax.Precision.HIGHEST, preferred_element_type=jnp.float32
    ).astype(jnp.bfloat16)
    return (gate_out, up_out, down_out, mixed)


def solution(mesh):
    in_specs = (
        P(("gr", "fs"), None),
        P(("gr", "fs"), None),
        P(("gr", "fs"), None),
        P(("gr", "fs")),
        P(None, ("gr", "fs"), "tp"),
        P(None, ("gr", "fs"), "tp"),
        P(None, ("gr", "fs"), "tp"),
    )
    out_specs = (
        P("fs", None, "tp"),
        P("fs", None, "tp"),
        P("fs", None, "tp"),
        P(("gr", "fs"), "tp"),
    )
    ng, nz, nt = mesh.shape["gr"], mesh.shape["fs"], mesh.shape["tp"]
    small = ng == 2 and nt == 4 and nz == 4
    work = functools.partial(fused, ng, nz, nt) if small else body
    return jax.shard_map(work, mesh=mesh, in_specs=in_specs, out_specs=out_specs, check_vma=False)
```

```python
import functools
import jax
import jax.numpy as jnp
from jax import lax
from jax.experimental import pallas as pl
from jax.experimental.pallas import tpu as pltpu
from jax.sharding import PartitionSpec as P

MESH = pl.DeviceIdType.MESH
VMEM_LIMIT = 50 * 1024 * 1024
EPSILON = 1e-05
BLOCKS = 4
LAG = 4


def kernel(ng, nz, nt, tok_in, routes, rweight, gain, gw, uw, dw, gout, uout, dout, mixed,
           tok, hid, part, crx, yrx, stage, raw, ret, rly, wsend, wrecv, wcol, gcol,
           ld, ts, tr, fs_s, fr, gs, gr, zs, zr, xs, xr, cs, cr, ys, yr, hs, hr, rs, rr):
    g, z, t = lax.axis_index("gr"), lax.axis_index("fs"), lax.axis_index("tp")
    core, y = lax.rem(t, 2), lax.div(t, 2)
    rows, d = tok_in.shape
    quarter = d // nt
    chunk, width = gw.shape[1], gw.shape[2]
    half = chunk // 2
    chunks = ng * nz
    per_owner = chunks // nt
    nb = BLOCKS
    blk = width // nb
    outs = (gout, uout)
    mate, over = y * 2 + 1 - core, (1 - y) * 2 + core
    inner = jnp.logical_and(z > 0, z < nz - 1)
    side = lax.div(z, 2)
    pair = z + 1 - 2 * lax.rem(z, 2)
    far = (3 * (1 - side), 2 - side)
    order = (far[0], far[1], pair, z)
    odd = lax.rem(z, 2)
    k_near = 3 - 2 * odd
    near_to = 4 - k_near
    k_mid = jnp.where(inner, near_to, 2)
    k_far = jnp.where(inner, 2, near_to)

    def to(k):
        return lax.rem(z + k, nz)

    def frm(k):
        return lax.rem(z + nz - k, nz)

    def rdma(src, dst, ss, rsem, dev):
        return pltpu.make_async_remote_copy(
            src_ref=src, dst_ref=dst, send_sem=ss, recv_sem=rsem, device_id=dev, device_id_type=MESH
        )

    def row0(group, zsrc):
        return pl.multiple_of((group * nz + zsrc) * chunk, chunk)

    def cols(b):
        return pl.ds(pl.multiple_of(b * blk, blk), blk)

    def qcols(q):
        return pl.ds(pl.multiple_of(q * quarter, quarter), quarter)

    def piece(m, b, group, zsrc):
        return outs[m].at[pl.ds(row0(group, zsrc), chunk), cols(b)]

    def dpiece(m, group, zsrc):
        return dout.at[pl.ds(pl.multiple_of(row0(group, zsrc) + m * half, half), half), :]

    def z_copy(m, b, k):
        return rdma(stage.at[m, to(k), :, cols(b)], piece(m, b, g, z), zs.at[m, b, k], zr.at[m, b, k], {"fs": to(k)})

    def zd_copy(m, k):
        return rdma(dw.at[to(k), pl.ds(m * half, half), :], dpiece(m, g, z), zs.at[m, nb, k], zr.at[m, nb, k], {"fs": to(k)})

    def x_own(m, b):
        return rdma(stage.at[m, z, :, cols(b)], piece(m, b, g, z), xs.at[m, b, 0], xr.at[m, b, 0], {"gr": 1 - g})

    def xd_own(m):
        return rdma(dw.at[z, pl.ds(m * half, half), :], dpiece(m, g, z), xs.at[m, nb, 0], xr.at[m, nb, 0], {"gr": 1 - g})

    def relay(ref, m, b, k):
        return rdma(ref, ref, xs.at[m, b, k], xr.at[m, b, k], {"gr": 1 - g})

    def z_arrive(ref, m, b, k):
        rdma(ref, ref, zs.at[m, b, k], zr.at[m, b, k], {"fs": to(k)}).wait_recv()

    def z_take(b, k):
        for m in range(2):
            ref = piece(m, b, g, frm(k))
            z_arrive(ref, m, b, k)
            relay(ref, m, b, k).start()

    def zd_take(k):
        for m in range(2):
            ref = dpiece(m, g, frm(k))
            z_arrive(ref, m, nb, k)
            relay(ref, m, nb, k).start()

    def order_of(j):
        return jnp.where(j == 0, far[0], jnp.where(j == 1, far[1], jnp.where(j == 2, pair, z)))

    def k_of(s):
        return jnp.where(s == 0, 0, jnp.where(s == 1, k_near, jnp.where(s == 2, k_far, k_mid)))

    def z_cross(b):
        for k in (2, k_near):
            for m in range(2):
                z_copy(m, b, k).start()

    def z_side(b):
        for m in range(2):
            z_copy(m, b, near_to).start()

    def z_down():
        for k in (near_to, 2, k_near):
            for m in range(2):
                zd_copy(m, k).start()

    load_tok = pltpu.make_async_copy(tok_in, raw, ld.at[0])
    loads = [pltpu.make_async_copy(src, stage.at[m], ld.at[1 + m]) for m, src in enumerate((gw, uw))]
    own_rows = pl.ds(row0(g, z), chunk)
    own_down = pltpu.make_async_copy(dw.at[z], dout.at[own_rows, :], ld.at[3])
    load_tok.start()
    for c in loads:
        c.start()
    own_down.start()

    barrier = pltpu.get_barrier_semaphore()
    for k in range(1, nz):
        pl.semaphore_signal(barrier, inc=1, device_id={"fs": to(k)}, device_id_type=MESH)
    for who in (mate, over):
        pl.semaphore_signal(barrier, inc=1, device_id={"tp": who}, device_id_type=MESH)
    pl.semaphore_signal(barrier, inc=1, device_id={"gr": 1 - g}, device_id_type=MESH)

    step = 64

    def norm():
        load_tok.wait()

        @pl.loop(0, rows // step)
        def _(i):
            at = pl.ds(pl.multiple_of(i * step, step), step)
            v = raw[at, :].astype(jnp.float32)
            scale = lax.rsqrt(jnp.mean(v * v, axis=-1, keepdims=True) + EPSILON)
            tok[z, at, :] = (v * scale).astype(jnp.bfloat16)

    norm()
    pl.semaphore_wait(barrier, nz - 1 + 3)

    guarded = []

    def guard(flag, c):
        @pl.when(flag)
        def _():
            c.start()
        guarded.append((flag, c))

    def hop(way, h, src):
        ref = tok.at[src, :, qcols(t)]
        nxt = lax.rem(z + way + nz, nz)
        return rdma(ref, ref, ts.at[(way + 1) // 2, h], tr.at[src], {"fs": nxt})

    right, left = z + 1 < nz, z >= 1
    guard(right, hop(1, 0, z))
    guard(left, hop(-1, 0, z))
    for m in range(2):
        xd_own(m).start()

    def scaleall():
        gcol[...] = jnp.transpose(jnp.broadcast_to(gain[...], (128, chunk)))
        for c in loads:
            c.wait()

        @pl.loop(0, nz * (chunk // step))
        def _(i):
            e = i // (chunk // step)
            at = pl.ds(pl.multiple_of(lax.rem(i, chunk // step) * step, step), step)
            factor = jnp.concatenate([gcol[at, :]] * (width // 128), axis=1)
            for m in range(2):
                stage[m, e, at, :] = (stage[m, e, at, :].astype(jnp.float32) * factor).astype(jnp.bfloat16)

    scaleall()
    @pl.when(jnp.logical_not(inner))
    def _():
        pl.loop(0, nb)(z_side)
        pl.loop(0, nb)(z_cross)

    @pl.when(inner)
    def _():
        z_side(0)

    for b in range(nb):
        for m in range(2):
            x_own(m, b).start()

    for e in range(nz):
        wsend[e] = (
            jnp.where(routes[0:1, :] == e, rweight[0:1, :], 0.0)
            + jnp.where(routes[1:2, :] == e, rweight[1:2, :], 0.0)
        )
    wrecv[z] = wsend[z]
    for k in range(1, nz):
        rdma(wsend.at[to(k)], wrecv.at[z], gs.at[k], gr.at[k], {"fs": to(k)}).start()
    for m in range(2):
        outs[m][own_rows, :] = stage[m, z]

    def hops(h):
        for way in (1, -1):
            src = lax.rem(z - way * h + nz, nz)
            valid = z >= h if way == 1 else z + h < nz
            more = right if way == 1 else left
            ref = tok.at[src, :, qcols(t)]

            @pl.when(valid)
            def _(ref=ref, src=src):
                rdma(ref, ref, ts.at[0, 0], tr.at[src], {"fs": lax.rem(z + 1, nz)}).wait_recv()
            guard(jnp.logical_and(valid, more), hop(way, h, src))
            guard(valid, rdma(ref, ref, fs_s.at[1, src], fr.at[1, src], {"tp": over}))
            guard(valid, rdma(ref, ref, fs_s.at[0, src], fr.at[0, src], {"tp": mate}))

    def take_near(lo, hi):
        @pl.loop(lo, hi)
        def _(b):
            z_take(b, k_near)

    hops(1)

    @pl.when(inner)
    def _():
        z_cross(0)
        take_near(0, nb // 2)
    hops(2)

    @pl.when(inner)
    def _():
        pl.loop(1, nb)(z_side)
        pl.loop(1, nb)(z_cross)
        z_down()
        take_near(nb // 2, nb)
    for h in range(3, nz):
        hops(h)

    z_take(0, k_mid)

    @pl.loop(0, nb)
    def _(b):
        z_take(b, k_far)

        @pl.when(jnp.logical_and(jnp.logical_not(inner), lax.rem(b, 2) == 0))
        def _():
            z_take(b // 2, k_near)

    def token_quarter(lane, src, q):
        ref = tok.at[src, :, qcols(q)]
        return rdma(ref, ref, fs_s.at[lane, src], fr.at[lane, src], {"tp": mate})

    def x_wait(b):
        @pl.loop(0, nz)
        def _(kk):
            for m in range(2):
                ref = piece(m, b, 1 - g, frm(kk))
                rdma(ref, ref, xs.at[m, b, kk], xr.at[m, b, kk], {"gr": 1 - g}).wait_recv()

    def tok_wait(src, s):
        token_quarter(1, src, over).wait_recv()
        token_quarter(2, src, over).start()
        token_quarter(0, src, mate).wait_recv()
        token_quarter(2, src, (1 - y) * 2 + 1 - core).wait_recv()
        rdma(wrecv.at[src], wrecv.at[src], gs.at[s], gr.at[s], {"fs": to(s)}).wait_recv()

    def hidden(b, src):
        a = tok[src]
        gate = jnp.dot(a, gout[:, cols(b)], preferred_element_type=jnp.float32)
        upper = jnp.dot(a, uout[:, cols(b)], preferred_element_type=jnp.float32)
        weight = jnp.concatenate([wcol[src]] * (blk // 128), axis=1)
        hid[src, :, cols(b)] = (gate / (1.0 + jnp.exp(-gate)) * upper * weight).astype(jnp.bfloat16)

    @pl.loop(nz, (nb + 1) * nz)
    def _(i):
        b, s = i // nz, lax.rem(i, nz)
        src = frm(k_of(s))

        @pl.when(jnp.logical_and(s == 0, b < nb))
        def _():
            z_take(b, k_mid)

        @pl.when(jnp.logical_and(jnp.logical_not(inner), jnp.logical_and(s == 1, b < (nb + 1) // 2 + 1)))
        def _():
            z_take(b + nb // 2 - 1, k_near)

        @pl.when(jnp.logical_and(jnp.logical_not(inner), i == (nb - 1) * nz))
        def _():
            z_down()

        @pl.when(s == 0)
        def _():
            x_wait(b - 1)

        @pl.when(b == 1)
        def _():
            @pl.when(s >= 1)
            def _():
                tok_wait(src, k_of(s))
            wcol[src] = jnp.transpose(jnp.broadcast_to(wrecv[src], (128, rows)))

        hidden(b - 1, src)

    own_down.wait()

    def chunk_of(i):
        k, other = k_of(i // 2), lax.rem(i, 2)
        group = g + other * (1 - 2 * g)
        c = group * nz + frm(k)
        owner = c // per_owner
        return k, other, c, owner, lax.rem(owner, 2), owner // 2, lax.rem(c, per_owner)

    def give(i, j):
        k, other, c, owner, par, yo, cc = chunk_of(i)
        b = order_of(j)
        return rdma(part.at[c, b], crx.at[yo * per_owner + cc, b], cs.at[i, j], cr.at[i, j], {"tp": mate})

    def up(i, j):
        k, other, c, owner, par, yo, cc = chunk_of(i)
        return rdma(part.at[c, order[j]], yrx.at[cc, order[j]], ys.at[i, j], yr.at[i, j], {"tp": over})

    def near(c, cc, j):
        dst = rly.at[j, cc] if j < 2 else ret.at[0, cc]
        return rdma(part.at[c, order[j]], dst, hs.at[j, cc], hr.at[j, cc], {"fs": pair})

    def cross(cc, j):
        return rdma(part.at[t * per_owner + cc, order[j]], ret.at[1, cc], rs.at[j, cc], rr.at[cc], {"fs": order[j]})

    def x_down_wait(k):
        for m in range(2):
            ref = dpiece(m, 1 - g, frm(k))
            rdma(ref, ref, xs.at[m, nb, k], xr.at[m, nb, k], {"gr": 1 - g}).wait_recv()

    def stage_a(i):
        k, other, c, owner, par, yo, cc = chunk_of(i)

        @pl.when(other == 1)
        def _():
            x_down_wait(k)

        mine = pl.ds(pl.multiple_of(c * chunk, chunk), chunk)

        @pl.loop(0, nz)
        def _(j):
            b = order_of(j)
            part[c, b] = lax.dot_general(
                hid[b], dout[mine, :], (((1,), (1,)), ((), ())), preferred_element_type=jnp.float32
            ).astype(jnp.bfloat16)

            @pl.when(par != core)
            def _():
                give(i, j).start()

    def stage_b(i):
        k, other, c, owner, par, yo, cc = chunk_of(i)

        @pl.when(par == core)
        def _():
            for j in range(nz):
                b = order[j]
                slot = crx.at[yo * per_owner + cc, b]
                rdma(slot, slot, cs.at[i, j], cr.at[i, j], {"tp": mate}).wait_recv()
                part[c, b] = (
                    part[c, b].astype(jnp.float32) + crx[yo * per_owner + cc, b].astype(jnp.float32)
                ).astype(jnp.bfloat16)

                @pl.when(yo != y)
                def _(j=j):
                    up(i, j).start()

    def stage_c(i):
        k, other, c, owner, par, yo, cc = chunk_of(i)

        @pl.when(owner == t)
        def _():
            for j in range(nz):
                b = order[j]
                slot = yrx.at[cc, b]
                rdma(slot, slot, ys.at[i, j], yr.at[i, j], {"tp": over}).wait_recv()
                part[c, b] = (
                    part[c, b].astype(jnp.float32) + yrx[cc, b].astype(jnp.float32)
                ).astype(jnp.bfloat16)
                if j < 2:
                    @pl.when(jnp.logical_not(inner))
                    def _(j=j):
                        near(c, cc, j).start()
                elif j == 2:
                    near(c, cc, j).start()

    n = chunks

    @pl.loop(0, n + LAG)
    def _(i):
        @pl.when(jnp.logical_or(i == 2, jnp.logical_or(i == 3, i == 5)))
        def _():
            zd_take(k_of((i + 1) // 2))

        @pl.when(i < n)
        def _():
            stage_a(i)
            stage_b(i)

        @pl.when(i >= LAG)
        def _():
            stage_c(i - LAG)

    def cross_phase():
        first = jnp.where(side == core, 0, 1)
        for turn in range(per_owner):
            cc = first + turn * (1 - 2 * first)
            for j in range(2):
                slot = rly.at[j, cc]
                rdma(slot, slot, hs.at[j, cc], hr.at[j, cc], {"fs": pair}).wait_recv()
                c, b = t * per_owner + cc, order[j]
                part[c, b] = (
                    part[c, b].astype(jnp.float32) + rly[j, cc].astype(jnp.float32)
                ).astype(jnp.bfloat16)
                cross(cc, j).start()

    pl.when(inner)(cross_phase)

    def final():
        for cc in range(per_owner):
            direct, crossed = ret.at[0, cc], ret.at[1, cc]
            rdma(direct, direct, hs.at[2, cc], hr.at[2, cc], {"fs": pair}).wait_recv()
            rdma(crossed, crossed, rs.at[0, cc], rr.at[cc], {"fs": pair}).wait_recv()
            mixed[:, cc * chunk:(cc + 1) * chunk] = (
                part[t * per_owner + cc, z].astype(jnp.float32)
                + ret[0, cc].astype(jnp.float32)
                + ret[1, cc].astype(jnp.float32)
            ).astype(jnp.bfloat16)

    final()

    def send_waits():
        @pl.loop(1, nz)
        def _(k):
            rdma(wsend.at[to(k)], wrecv.at[z], gs.at[k], gr.at[k], {"fs": to(k)}).wait_send()
            for m in range(2):
                zd_copy(m, k).wait_send()
                relay(dpiece(m, g, frm(k)), m, nb, k).wait_send()
            token_quarter(2, frm(k), over).wait_send()

            @pl.loop(0, nb)
            def _(b):
                for m in range(2):
                    z_copy(m, b, k).wait_send()
                    relay(piece(m, b, g, frm(k)), m, b, k).wait_send()

        for m in range(2):
            xd_own(m).wait_send()

            @pl.loop(0, nb)
            def _(b):
                x_own(m, b).wait_send()

        for flag, c in guarded:
            @pl.when(flag)
            def _(c=c):
                c.wait_send()

        @pl.loop(0, n)
        def _(i):
            k, other, c, owner, par, yo, cc = chunk_of(i)

            @pl.when(par != core)
            def _():
                for j in range(nz):
                    give(i, j).wait_send()

            @pl.when(jnp.logical_and(par == core, yo != y))
            def _():
                for j in range(nz):
                    up(i, j).wait_send()

        for cc in range(per_owner):
            c = t * per_owner + cc
            near(c, cc, 2).wait_send()
            for j in range(2):
                @pl.when(inner)
                def _(j=j, cc=cc):
                    cross(cc, j).wait_send()

                @pl.when(jnp.logical_not(inner))
                def _(j=j, c=c, cc=cc):
                    near(c, cc, j).wait_send()

    send_waits()


def store(gate, upper, down, mixed, gate_out, up_out, down_out, mixed_out, sem):
    copies = [
        pltpu.make_async_copy(gate, gate_out.at[0], sem.at[0]),
        pltpu.make_async_copy(upper, up_out.at[0], sem.at[1]),
        pltpu.make_async_copy(down, down_out.at[0], sem.at[2]),
        pltpu.make_async_copy(mixed, mixed_out, sem.at[3]),
    ]
    for c in copies:
        c.start()
    for c in copies:
        c.wait()


def fused(ng, nz, nt, tokens, routes, route_weight, gain, w_gate, w_up, w_down):
    rows, d = tokens.shape
    quarter = d // nt
    experts, chunk, width = w_gate.shape
    chunks = ng * nz
    per_owner = chunks // nt
    bf, f32 = jnp.bfloat16, jnp.float32
    dma = pltpu.SemaphoreType.DMA
    full = pltpu.VMEM((d, width), bf)
    vmem = pl.BlockSpec(memory_space=pltpu.VMEM)
    anywhere = pl.BlockSpec(memory_space=pl.ANY)
    results = pl.pallas_call(
        functools.partial(kernel, ng, nz, nt),
        out_shape=(full, full, full, pltpu.VMEM((rows, quarter), bf)),
        in_specs=[anywhere, vmem, vmem, vmem, anywhere, anywhere, anywhere],
        out_specs=(vmem,) * 4,
        scratch_shapes=[
            pltpu.VMEM((nz, rows, d), bf),
            pltpu.VMEM((nz, rows, width), bf),
            pltpu.VMEM((chunks, nz, rows, chunk), bf),
            pltpu.VMEM((chunks // 2, nz, rows, chunk), bf),
            pltpu.VMEM((per_owner, nz, rows, chunk), bf),
            pltpu.VMEM((2, nz, chunk, width), bf),
            pltpu.VMEM((rows, d), bf),
            pltpu.VMEM((2, per_owner, rows, chunk), bf),
            pltpu.VMEM((2, per_owner, rows, chunk), bf),
            pltpu.VMEM((nz, 1, rows), f32),
            pltpu.VMEM((nz, 1, rows), f32),
            pltpu.VMEM((nz, rows, 128), f32),
            pltpu.VMEM((chunk, 128), f32),
            dma((4,)),
            dma((2, nz)), dma((nz,)),
            dma((3, nz)), dma((3, nz)),
            dma((nz,)), dma((nz,)),
            dma((2, BLOCKS + 1, nz)), dma((2, BLOCKS + 1, nz)),
            dma((2, BLOCKS + 1, nz)), dma((2, BLOCKS + 1, nz)),
            dma((chunks, nz)), dma((chunks, nz)),
            dma((chunks, nz)), dma((chunks, nz)),
            dma((3, per_owner)), dma((3, per_owner)),
            dma((2, per_owner)), dma((per_owner,)),
        ],
        compiler_params=pltpu.CompilerParams(
            collective_id=0, has_side_effects=True, vmem_limit_bytes=VMEM_LIMIT
        ),
    )(tokens, routes.T, route_weight.T, gain.reshape(1, chunk), w_gate, w_up, w_down)
    whole = jax.ShapeDtypeStruct((1, d, width), bf)
    return pl.pallas_call(
        store,
        out_shape=(whole, whole, whole, jax.ShapeDtypeStruct((rows, quarter), bf)),
        in_specs=[vmem] * 4,
        out_specs=(anywhere,) * 4,
        scratch_shapes=[dma((4,))],
        compiler_params=pltpu.CompilerParams(vmem_limit_bytes=4 * 1024 * 1024),
    )(*results)

EXP_DEV = 1


def body(tokens, routes, route_weight, gain, w_gate, w_up, w_down):
    scaling = gain[None, :, None]
    gate_local = (w_gate * scaling).astype(jnp.bfloat16)
    up_local = (w_up * scaling).astype(jnp.bfloat16)
    gate_mine, up_mine, down_mine = (
        lax.all_to_all(gate_local, "fs", split_axis=0, concat_axis=1, tiled=True),
        lax.all_to_all(up_local, "fs", split_axis=0, concat_axis=1, tiled=True),
        lax.all_to_all(w_down, "fs", split_axis=0, concat_axis=1, tiled=True),
    )
    gate_out, up_out, down_out = (
        lax.all_gather(gate_mine, "gr", axis=1, tiled=True),
        lax.all_gather(up_mine, "gr", axis=1, tiled=True),
        lax.all_gather(down_mine, "gr", axis=1, tiled=True),
    )
    fs_count = lax.axis_size("fs")
    experts = EXP_DEV * fs_count
    tok_rows = tokens.shape[0]
    capacity = 3 * tok_rows // experts
    float_rows = tokens.astype(jnp.float32)
    normed = (
        float_rows * lax.rsqrt(jnp.mean(float_rows * float_rows, axis=-1, keepdims=True) + EPSILON)
    ).astype(jnp.bfloat16)
    flat_ids = routes.reshape(-1)
    onehot = (flat_ids[:, None] == jnp.arange(experts, dtype=jnp.int32)[None, :]).astype(jnp.int32)
    slot_rank = jnp.sum((jnp.cumsum(onehot, axis=0) - onehot) * onehot, axis=-1)
    destination = (flat_ids * capacity + slot_rank).reshape(tok_rows, 2)
    slot_ids = jnp.arange(experts * capacity, dtype=jnp.int32)
    hits = slot_ids[:, None, None] == destination[None, :, :]
    dispatch = jnp.any(hits, axis=-1).astype(jnp.bfloat16)
    outgoing = jnp.dot(dispatch, normed, preferred_element_type=jnp.float32).astype(jnp.bfloat16)
    outgoing = outgoing.reshape(fs_count, EXP_DEV, capacity, tokens.shape[1])
    arrived = lax.all_to_all(outgoing, "fs", split_axis=0, concat_axis=0, tiled=True)
    gate = jnp.einsum("sjnd,jdf->sjnf", arrived, gate_out, preferred_element_type=jnp.float32)
    upper = jnp.einsum("sjnd,jdf->sjnf", arrived, up_out, preferred_element_type=jnp.float32)
    hidden = (jax.nn.silu(gate) * upper).astype(jnp.bfloat16)
    partial_value = jnp.einsum(
        "sjnf,jdf->sjnd", hidden, down_out, preferred_element_type=jnp.float32
    )
    rounded = lax.optimization_barrier(partial_value.astype(jnp.bfloat16))
    summed = lax.psum_scatter(
        rounded.astype(jnp.float32).astype(jnp.bfloat16), "tp", scatter_dimension=3, tiled=True
    )
    back_home = lax.all_to_all(summed, "fs", split_axis=0, concat_axis=0, tiled=True)
    features = back_home.shape[-1]
    flat_back = back_home.reshape(experts * capacity, features).astype(jnp.float32)
    first = jnp.where(slot_ids[None, :] == destination[:, 0:1], route_weight[:, 0:1], 0.0)
    second = jnp.where(slot_ids[None, :] == destination[:, 1:2], route_weight[:, 1:2], 0.0)
    combine_map = first + second
    mixed = jnp.dot(
        combine_map, flat_back, precision=lax.Precision.HIGHEST, preferred_element_type=jnp.float32
    ).astype(jnp.bfloat16)
    return (gate_out, up_out, down_out, mixed)


def solution(mesh):
    in_specs = (
        P(("gr", "fs"), None),
        P(("gr", "fs"), None),
        P(("gr", "fs"), None),
        P(("gr", "fs")),
        P(None, ("gr", "fs"), "tp"),
        P(None, ("gr", "fs"), "tp"),
        P(None, ("gr", "fs"), "tp"),
    )
    out_specs = (
        P("fs", None, "tp"),
        P("fs", None, "tp"),
        P("fs", None, "tp"),
        P(("gr", "fs"), "tp"),
    )
    ng, nz, nt = mesh.shape["gr"], mesh.shape["fs"], mesh.shape["tp"]
    small = ng == 2 and nt == 4 and nz == 4
    work = functools.partial(fused, ng, nz, nt) if small else body
    return jax.shard_map(work, mesh=mesh, in_specs=in_specs, out_specs=out_specs, check_vma=False)
```

```python
import functools
import jax
import jax.numpy as jnp
from jax import lax
from jax.experimental import pallas as pl
from jax.experimental.pallas import tpu as pltpu
from jax.sharding import PartitionSpec as P

MESH = pl.DeviceIdType.MESH
VMEM_LIMIT = 50 * 1024 * 1024
EPSILON = 1e-05
BLOCKS = 4
LAG = 4


def kernel(ng, nz, nt, tok_in, routes, rweight, gain, gw, uw, dw, gout, uout, dout, mixed,
           tok, hid, part, crx, yrx, stage, raw, ret, rly, wsend, wrecv, wcol, gcol,
           ld, ts, tr, fs_s, fr, gs, gr, zs, zr, xs, xr, cs, cr, ys, yr, hs, hr, rs, rr):
    g, z, t = lax.axis_index("gr"), lax.axis_index("fs"), lax.axis_index("tp")
    core, y = lax.rem(t, 2), lax.div(t, 2)
    rows, d = tok_in.shape
    quarter = d // nt
    chunk, width = gw.shape[1], gw.shape[2]
    half = chunk // 2
    chunks = ng * nz
    per_owner = chunks // nt
    nb = BLOCKS
    blk = width // nb
    outs = (gout, uout)
    mate, over = y * 2 + 1 - core, (1 - y) * 2 + core
    inner = jnp.logical_and(z > 0, z < nz - 1)
    side = lax.div(z, 2)
    pair = z + 1 - 2 * lax.rem(z, 2)
    far = (3 * (1 - side), 2 - side)
    order = (far[0], far[1], pair, z)
    odd = lax.rem(z, 2)
    k_near = 3 - 2 * odd
    near_to = 4 - k_near
    k_mid = jnp.where(inner, near_to, 2)
    k_far = jnp.where(inner, 2, near_to)

    def to(k):
        return lax.rem(z + k, nz)

    def frm(k):
        return lax.rem(z + nz - k, nz)

    def rdma(src, dst, ss, rsem, dev):
        return pltpu.make_async_remote_copy(
            src_ref=src, dst_ref=dst, send_sem=ss, recv_sem=rsem, device_id=dev, device_id_type=MESH
        )

    def row0(group, zsrc):
        return pl.multiple_of((group * nz + zsrc) * chunk, chunk)

    def cols(b):
        return pl.ds(pl.multiple_of(b * blk, blk), blk)

    def qcols(q):
        return pl.ds(pl.multiple_of(q * quarter, quarter), quarter)

    def piece(m, b, group, zsrc):
        return outs[m].at[pl.ds(row0(group, zsrc), chunk), cols(b)]

    def dpiece(m, group, zsrc):
        return dout.at[pl.ds(pl.multiple_of(row0(group, zsrc) + m * half, half), half), :]

    def z_copy(m, b, k):
        return rdma(stage.at[m, to(k), :, cols(b)], piece(m, b, g, z), zs.at[m, b, k], zr.at[m, b, k], {"fs": to(k)})

    def zd_copy(m, k):
        return rdma(dw.at[to(k), pl.ds(m * half, half), :], dpiece(m, g, z), zs.at[m, nb, k], zr.at[m, nb, k], {"fs": to(k)})

    def x_own(m, b):
        return rdma(stage.at[m, z, :, cols(b)], piece(m, b, g, z), xs.at[m, b, 0], xr.at[m, b, 0], {"gr": 1 - g})

    def xd_own(m):
        return rdma(dw.at[z, pl.ds(m * half, half), :], dpiece(m, g, z), xs.at[m, nb, 0], xr.at[m, nb, 0], {"gr": 1 - g})

    def relay(ref, m, b, k):
        return rdma(ref, ref, xs.at[m, b, k], xr.at[m, b, k], {"gr": 1 - g})

    def z_arrive(ref, m, b, k):
        rdma(ref, ref, zs.at[m, b, k], zr.at[m, b, k], {"fs": to(k)}).wait_recv()

    def z_take(b, k):
        for m in range(2):
            ref = piece(m, b, g, frm(k))
            z_arrive(ref, m, b, k)
            relay(ref, m, b, k).start()

    def zd_take(k, ms=(0, 1)):
        for m in ms:
            ref = dpiece(m, g, frm(k))
            z_arrive(ref, m, nb, k)
            relay(ref, m, nb, k).start()

    def order_of(j):
        return jnp.where(j == 0, far[0], jnp.where(j == 1, far[1], jnp.where(j == 2, pair, z)))

    def k_of(s):
        return jnp.where(s == 0, 0, jnp.where(s == 1, k_near, jnp.where(s == 2, k_far, k_mid)))

    def z_cross(b, ms=(0, 1)):
        for m in ms:
            for k in (2, k_near):
                z_copy(m, b, k).start()

    def z_side(b):
        for m in range(2):
            z_copy(m, b, near_to).start()

    def z_down():
        for m in range(2):
            zd_copy(m, near_to).start()
        for m in range(2):
            for k in (2, k_near):
                zd_copy(m, k).start()

    load_tok = pltpu.make_async_copy(tok_in, raw, ld.at[0])
    loads = [pltpu.make_async_copy(src, stage.at[m], ld.at[1 + m]) for m, src in enumerate((gw, uw))]
    own_rows = pl.ds(row0(g, z), chunk)
    own_down = pltpu.make_async_copy(dw.at[z], dout.at[own_rows, :], ld.at[3])
    load_tok.start()
    for c in loads:
        c.start()
    own_down.start()

    barrier = pltpu.get_barrier_semaphore()
    for k in range(1, nz):
        pl.semaphore_signal(barrier, inc=1, device_id={"fs": to(k)}, device_id_type=MESH)
    for who in (mate, over):
        pl.semaphore_signal(barrier, inc=1, device_id={"tp": who}, device_id_type=MESH)
    pl.semaphore_signal(barrier, inc=1, device_id={"gr": 1 - g}, device_id_type=MESH)

    step = 64

    def norm():
        load_tok.wait()

        @pl.loop(0, rows // step)
        def _(i):
            at = pl.ds(pl.multiple_of(i * step, step), step)
            v = raw[at, :].astype(jnp.float32)
            scale = lax.rsqrt(jnp.mean(v * v, axis=-1, keepdims=True) + EPSILON)
            tok[z, at, :] = (v * scale).astype(jnp.bfloat16)

    norm()
    pl.semaphore_wait(barrier, nz - 1 + 3)

    guarded = []

    def guard(flag, c):
        @pl.when(flag)
        def _():
            c.start()
        guarded.append((flag, c))

    def hop(way, h, src):
        ref = tok.at[src, :, qcols(t)]
        nxt = lax.rem(z + way + nz, nz)
        return rdma(ref, ref, ts.at[(way + 1) // 2, h], tr.at[src], {"fs": nxt})

    right, left = z + 1 < nz, z >= 1
    guard(right, hop(1, 0, z))
    guard(left, hop(-1, 0, z))
    for m in range(2):
        xd_own(m).start()

    def scaleall():
        gcol[...] = jnp.transpose(jnp.broadcast_to(gain[...], (128, chunk)))
        for c in loads:
            c.wait()

        @pl.loop(0, nz * (chunk // step))
        def _(i):
            e = i // (chunk // step)
            at = pl.ds(pl.multiple_of(lax.rem(i, chunk // step) * step, step), step)
            factor = jnp.concatenate([gcol[at, :]] * (width // 128), axis=1)
            for m in range(2):
                stage[m, e, at, :] = (stage[m, e, at, :].astype(jnp.float32) * factor).astype(jnp.bfloat16)

    scaleall()
    @pl.when(jnp.logical_not(inner))
    def _():
        pl.loop(0, nb)(z_side)
        pl.loop(0, nb)(z_cross)

    @pl.when(inner)
    def _():
        z_side(0)
        z_cross(0, (0,))

    for b in range(nb):
        for m in range(2):
            x_own(m, b).start()

    for e in range(nz):
        wsend[e] = (
            jnp.where(routes[0:1, :] == e, rweight[0:1, :], 0.0)
            + jnp.where(routes[1:2, :] == e, rweight[1:2, :], 0.0)
        )
    wrecv[z] = wsend[z]
    for k in range(1, nz):
        rdma(wsend.at[to(k)], wrecv.at[z], gs.at[k], gr.at[k], {"fs": to(k)}).start()
    for m in range(2):
        outs[m][own_rows, :] = stage[m, z]

    def hops(h):
        for way in (1, -1):
            src = lax.rem(z - way * h + nz, nz)
            valid = z >= h if way == 1 else z + h < nz
            more = right if way == 1 else left
            ref = tok.at[src, :, qcols(t)]

            @pl.when(valid)
            def _(ref=ref, src=src):
                rdma(ref, ref, ts.at[0, 0], tr.at[src], {"fs": lax.rem(z + 1, nz)}).wait_recv()
            guard(jnp.logical_and(valid, more), hop(way, h, src))
            guard(valid, rdma(ref, ref, fs_s.at[1, src], fr.at[1, src], {"tp": over}))
            guard(valid, rdma(ref, ref, fs_s.at[0, src], fr.at[0, src], {"tp": mate}))

    def take_near(lo, hi):
        @pl.loop(lo, hi)
        def _(b):
            z_take(b, k_near)

    hops(1)

    @pl.when(inner)
    def _():
        z_cross(0, (1,))
        take_near(0, nb // 2)
    hops(2)

    @pl.when(inner)
    def _():
        pl.loop(1, nb)(z_side)
        pl.loop(1, nb)(z_cross)
        z_down()
        take_near(nb // 2, nb)
    for h in range(3, nz):
        hops(h)

    z_take(0, k_mid)

    @pl.loop(0, nb)
    def _(b):
        z_take(b, k_far)

        @pl.when(jnp.logical_and(jnp.logical_not(inner), lax.rem(b, 2) == 0))
        def _():
            z_take(b // 2, k_near)

    def token_quarter(lane, src, q):
        ref = tok.at[src, :, qcols(q)]
        return rdma(ref, ref, fs_s.at[lane, src], fr.at[lane, src], {"tp": mate})

    def x_wait(b):
        @pl.loop(0, nz)
        def _(kk):
            for m in range(2):
                ref = piece(m, b, 1 - g, frm(kk))
                rdma(ref, ref, xs.at[m, b, kk], xr.at[m, b, kk], {"gr": 1 - g}).wait_recv()

    def tok_wait(src, s):
        token_quarter(1, src, over).wait_recv()
        token_quarter(2, src, over).start()
        token_quarter(0, src, mate).wait_recv()
        token_quarter(2, src, (1 - y) * 2 + 1 - core).wait_recv()
        rdma(wrecv.at[src], wrecv.at[src], gs.at[s], gr.at[s], {"fs": to(s)}).wait_recv()

    def hidden(b, src):
        a = tok[src]
        gate = jnp.dot(a, gout[:, cols(b)], preferred_element_type=jnp.float32)
        upper = jnp.dot(a, uout[:, cols(b)], preferred_element_type=jnp.float32)
        weight = jnp.concatenate([wcol[src]] * (blk // 128), axis=1)
        hid[src, :, cols(b)] = (gate / (1.0 + jnp.exp(-gate)) * upper * weight).astype(jnp.bfloat16)

    @pl.loop(nz, (nb + 1) * nz)
    def _(i):
        b, s = i // nz, lax.rem(i, nz)
        src = frm(k_of(s))

        @pl.when(jnp.logical_and(s == 0, b < nb))
        def _():
            z_take(b, k_mid)

        @pl.when(jnp.logical_and(jnp.logical_not(inner), jnp.logical_and(s == 1, b < (nb + 1) // 2 + 1)))
        def _():
            z_take(b + nb // 2 - 1, k_near)

        @pl.when(jnp.logical_and(jnp.logical_not(inner), i == (nb - 1) * nz))
        def _():
            z_down()

        @pl.when(s == 0)
        def _():
            x_wait(b - 1)

        @pl.when(b == 1)
        def _():
            @pl.when(s >= 1)
            def _():
                tok_wait(src, k_of(s))
            wcol[src] = jnp.transpose(jnp.broadcast_to(wrecv[src], (128, rows)))

        hidden(b - 1, src)

    own_down.wait()

    def chunk_of(i):
        k, other = k_of(i // 2), lax.rem(i, 2)
        group = g + other * (1 - 2 * g)
        c = group * nz + frm(k)
        owner = c // per_owner
        return k, other, c, owner, lax.rem(owner, 2), owner // 2, lax.rem(c, per_owner)

    def cut(ref, h):
        return ref if h is None else ref.at[:, pl.ds(h * half, half)]

    def slot_of(i, h):
        return i + 2 if h == 1 else i

    def give(i, j, h):
        k, other, c, owner, par, yo, cc = chunk_of(i)
        b, si = order_of(j), slot_of(i, h)
        src, dst = cut(part.at[c, b], h), cut(crx.at[yo * per_owner + cc, b], h)
        return rdma(src, dst, cs.at[si, j], cr.at[si, j], {"tp": mate})

    def up(i, j, h):
        k, other, c, owner, par, yo, cc = chunk_of(i)
        si = slot_of(i, h)
        src, dst = cut(part.at[c, order[j]], h), cut(yrx.at[cc, order[j]], h)
        return rdma(src, dst, ys.at[si, j], yr.at[si, j], {"tp": over})

    def near(c, cc, j, h):
        second = 1 if h == 1 else 0
        dst = rly.at[j, cc] if j < 2 else ret.at[0, cc]
        landed = hr.at[j, cc, second if j < 2 else 0]
        return rdma(cut(part.at[c, order[j]], h), cut(dst, h), hs.at[j, cc, second], landed, {"fs": pair})

    def cross(cc, j, h):
        second = 1 if h == 1 else 0
        src, dst = cut(part.at[t * per_owner + cc, order[j]], h), cut(ret.at[1, cc], h)
        return rdma(src, dst, rs.at[j, cc, second], rr.at[cc], {"fs": order[j]})

    def x_down_wait(k, ms):
        for m in ms:
            ref = dpiece(m, 1 - g, frm(k))
            rdma(ref, ref, xs.at[m, nb, k], xr.at[m, nb, k], {"gr": 1 - g}).wait_recv()

    def stage_a(i):
        k, other, c, owner, par, yo, cc = chunk_of(i)

        @pl.when(other == 1)
        def _():
            x_down_wait(k, range(2))
        mine = pl.ds(pl.multiple_of(c * chunk, chunk), chunk)

        @pl.loop(0, nz)
        def _(j):
            b = order_of(j)
            part[c, b] = lax.dot_general(
                hid[b], dout[mine, :], (((1,), (1,)), ((), ())), preferred_element_type=jnp.float32
            ).astype(jnp.bfloat16)

            @pl.when(par != core)
            def _():
                give(i, j, None).start()

    def halves_a(i, h):
        k, other, c, owner, par, yo, cc = chunk_of(i)
        c2 = chunk_of(i + 1)[2]
        x_down_wait(k, (h,))
        mine = [pl.ds(pl.multiple_of(v * chunk + h * half, half), half) for v in (c, c2)]

        @pl.loop(0, nz)
        def _(j):
            b = order_of(j)
            both = lax.dot_general(
                hid[b], jnp.concatenate([dout[v, :] for v in mine], axis=0), (((1,), (1,)), ((), ())),
                preferred_element_type=jnp.float32,
            ).astype(jnp.bfloat16)
            cut(part.at[c, b], h)[...] = both[:, :half]
            cut(part.at[c2, b], h)[...] = both[:, half:]

            @pl.when(par != core)
            def _():
                give(i, j, h).start()
                give(i + 1, j, h).start()

    def add(c, b, h, ref):
        mine = cut(part.at[c, b], h)
        mine[...] = (mine[...].astype(jnp.float32) + ref[...].astype(jnp.float32)).astype(jnp.bfloat16)

    def stage_b(i, h=None):
        k, other, c, owner, par, yo, cc = chunk_of(i)
        si = slot_of(i, h)

        @pl.when(par == core)
        def _():
            for j in range(nz):
                b = order[j]
                ref = cut(crx.at[yo * per_owner + cc, b], h)
                rdma(ref, ref, cs.at[si, j], cr.at[si, j], {"tp": mate}).wait_recv()
                add(c, b, h, ref)

                @pl.when(yo != y)
                def _(j=j):
                    up(i, j, h).start()

    def stage_c(i, h=None):
        k, other, c, owner, par, yo, cc = chunk_of(i)
        si = slot_of(i, h)

        @pl.when(owner == t)
        def _():
            for j in range(nz):
                b = order[j]
                ref = cut(yrx.at[cc, b], h)
                rdma(ref, ref, ys.at[si, j], yr.at[si, j], {"tp": over}).wait_recv()
                add(c, b, h, ref)
                if j < 2:
                    @pl.when(jnp.logical_not(inner))
                    def _(j=j):
                        near(c, cc, j, h).start()
                elif j == 2:
                    near(c, cc, j, h).start()

    def cross_phase(cc, h=None):
        for j in range(2):
            ref = cut(rly.at[j, cc], h)
            rdma(ref, ref, hs.at[j, cc, 0], hr.at[j, cc, 1 if h == 1 else 0], {"fs": pair}).wait_recv()
            add(t * per_owner + cc, order[j], h, ref)
            cross(cc, j, h).start()

    n = chunks
    early = jnp.logical_and(inner, side == core)
    late = jnp.logical_and(inner, side != core)
    cc_far = lax.rem(frm(k_far), 2)
    zd_take(k_near)

    @pl.loop(0, n - 2)
    def _(i):
        @pl.when(i == 2)
        def _():
            zd_take(k_far, (0,))

        @pl.when(i == 4)
        def _():
            zd_take(k_far, (1,))
            pl.loop(0, 2)(stage_c)
            zd_take(k_mid, (0,))

        stage_a(i)
        stage_b(i)

    pl.loop(2, 4)(stage_c)

    def last(h):
        halves_a(n - 2, h)

        @pl.loop(n - 2, n)
        def _(i):
            stage_b(i, h)

    last(0)
    zd_take(k_mid, (1,))

    @pl.when(early)
    def _():
        pl.loop(0, per_owner)(cross_phase)
    pl.loop(n - 4, n - 2)(stage_c)
    last(1)

    @pl.when(late)
    def _():
        cross_phase(cc_far)
    for h in range(2):
        @pl.loop(n - 2, n)
        def _(i, h=h):
            stage_c(i, h)

        @pl.when(late)
        def _(h=h):
            cross_phase(1 - cc_far, h)

    def final():
        for cc in range(per_owner):
            direct, crossed = ret.at[0, cc], ret.at[1, cc]
            rdma(direct, direct, hs.at[2, cc, 0], hr.at[2, cc, 0], {"fs": pair}).wait_recv()
            rdma(crossed, crossed, rs.at[0, cc, 0], rr.at[cc], {"fs": pair}).wait_recv()
            mixed[:, cc * chunk:(cc + 1) * chunk] = (
                part[t * per_owner + cc, z].astype(jnp.float32)
                + ret[0, cc].astype(jnp.float32)
                + ret[1, cc].astype(jnp.float32)
            ).astype(jnp.bfloat16)

    final()

    def send_waits():
        @pl.loop(1, nz)
        def _(k):
            rdma(wsend.at[to(k)], wrecv.at[z], gs.at[k], gr.at[k], {"fs": to(k)}).wait_send()
            for m in range(2):
                zd_copy(m, k).wait_send()
                relay(dpiece(m, g, frm(k)), m, nb, k).wait_send()
            token_quarter(2, frm(k), over).wait_send()

            @pl.loop(0, nb)
            def _(b):
                for m in range(2):
                    z_copy(m, b, k).wait_send()
                    relay(piece(m, b, g, frm(k)), m, b, k).wait_send()

        for m in range(2):
            xd_own(m).wait_send()

            @pl.loop(0, nb)
            def _(b):
                x_own(m, b).wait_send()

        for flag, c in guarded:
            @pl.when(flag)
            def _(c=c):
                c.wait_send()

        def sent(i, h):
            k, other, c, owner, par, yo, cc = chunk_of(i)

            @pl.when(par != core)
            def _():
                for j in range(nz):
                    give(i, j, h).wait_send()

            @pl.when(jnp.logical_and(par == core, yo != y))
            def _():
                for j in range(nz):
                    up(i, j, h).wait_send()

        def returned(cc, h):
            c = t * per_owner + cc
            near(c, cc, 2, h).wait_send()
            for j in range(2):
                @pl.when(inner)
                def _(j=j):
                    cross(cc, j, h).wait_send()

                @pl.when(jnp.logical_not(inner))
                def _(j=j):
                    near(c, cc, j, h).wait_send()

        @pl.loop(0, n - 2)
        def _(i):
            sent(i, None)
        for h in range(2):
            @pl.loop(n - 2, n)
            def _(i, h=h):
                sent(i, h)
        returned(cc_far, None)

        @pl.when(side == core)
        def _():
            returned(1 - cc_far, None)

        @pl.when(side != core)
        def _():
            for h in range(2):
                returned(1 - cc_far, h)

    send_waits()


def store(gate, upper, down, mixed, gate_out, up_out, down_out, mixed_out, sem):
    copies = [
        pltpu.make_async_copy(gate, gate_out.at[0], sem.at[0]),
        pltpu.make_async_copy(upper, up_out.at[0], sem.at[1]),
        pltpu.make_async_copy(down, down_out.at[0], sem.at[2]),
        pltpu.make_async_copy(mixed, mixed_out, sem.at[3]),
    ]
    for c in copies:
        c.start()
    for c in copies:
        c.wait()


def fused(ng, nz, nt, tokens, routes, route_weight, gain, w_gate, w_up, w_down):
    rows, d = tokens.shape
    quarter = d // nt
    experts, chunk, width = w_gate.shape
    chunks = ng * nz
    per_owner = chunks // nt
    bf, f32 = jnp.bfloat16, jnp.float32
    dma = pltpu.SemaphoreType.DMA
    full = pltpu.VMEM((d, width), bf)
    vmem = pl.BlockSpec(memory_space=pltpu.VMEM)
    anywhere = pl.BlockSpec(memory_space=pl.ANY)
    results = pl.pallas_call(
        functools.partial(kernel, ng, nz, nt),
        out_shape=(full, full, full, pltpu.VMEM((rows, quarter), bf)),
        in_specs=[anywhere, vmem, vmem, vmem, anywhere, anywhere, anywhere],
        out_specs=(vmem,) * 4,
        scratch_shapes=[
            pltpu.VMEM((nz, rows, d), bf),
            pltpu.VMEM((nz, rows, width), bf),
            pltpu.VMEM((chunks, nz, rows, chunk), bf),
            pltpu.VMEM((chunks // 2, nz, rows, chunk), bf),
            pltpu.VMEM((per_owner, nz, rows, chunk), bf),
            pltpu.VMEM((2, nz, chunk, width), bf),
            pltpu.VMEM((rows, d), bf),
            pltpu.VMEM((2, per_owner, rows, chunk), bf),
            pltpu.VMEM((2, per_owner, rows, chunk), bf),
            pltpu.VMEM((nz, 1, rows), f32),
            pltpu.VMEM((nz, 1, rows), f32),
            pltpu.VMEM((nz, rows, 128), f32),
            pltpu.VMEM((chunk, 128), f32),
            dma((4,)),
            dma((2, nz)), dma((nz,)),
            dma((3, nz)), dma((3, nz)),
            dma((nz,)), dma((nz,)),
            dma((2, BLOCKS + 1, nz)), dma((2, BLOCKS + 1, nz)),
            dma((2, BLOCKS + 1, nz)), dma((2, BLOCKS + 1, nz)),
            dma((chunks + 2, nz)), dma((chunks + 2, nz)),
            dma((chunks + 2, nz)), dma((chunks + 2, nz)),
            dma((3, per_owner, 2)), dma((3, per_owner, 2)),
            dma((2, per_owner, 2)), dma((per_owner,)),
        ],
        compiler_params=pltpu.CompilerParams(
            collective_id=0, has_side_effects=True, vmem_limit_bytes=VMEM_LIMIT
        ),
    )(tokens, routes.T, route_weight.T, gain.reshape(1, chunk), w_gate, w_up, w_down)
    whole = jax.ShapeDtypeStruct((1, d, width), bf)
    return pl.pallas_call(
        store,
        out_shape=(whole, whole, whole, jax.ShapeDtypeStruct((rows, quarter), bf)),
        in_specs=[vmem] * 4,
        out_specs=(anywhere,) * 4,
        scratch_shapes=[dma((4,))],
        compiler_params=pltpu.CompilerParams(vmem_limit_bytes=4 * 1024 * 1024),
    )(*results)

EXP_DEV = 1


def body(tokens, routes, route_weight, gain, w_gate, w_up, w_down):
    scaling = gain[None, :, None]
    gate_local = (w_gate * scaling).astype(jnp.bfloat16)
    up_local = (w_up * scaling).astype(jnp.bfloat16)
    gate_mine, up_mine, down_mine = (
        lax.all_to_all(gate_local, "fs", split_axis=0, concat_axis=1, tiled=True),
        lax.all_to_all(up_local, "fs", split_axis=0, concat_axis=1, tiled=True),
        lax.all_to_all(w_down, "fs", split_axis=0, concat_axis=1, tiled=True),
    )
    gate_out, up_out, down_out = (
        lax.all_gather(gate_mine, "gr", axis=1, tiled=True),
        lax.all_gather(up_mine, "gr", axis=1, tiled=True),
        lax.all_gather(down_mine, "gr", axis=1, tiled=True),
    )
    fs_count = lax.axis_size("fs")
    experts = EXP_DEV * fs_count
    tok_rows = tokens.shape[0]
    capacity = 3 * tok_rows // experts
    float_rows = tokens.astype(jnp.float32)
    normed = (
        float_rows * lax.rsqrt(jnp.mean(float_rows * float_rows, axis=-1, keepdims=True) + EPSILON)
    ).astype(jnp.bfloat16)
    flat_ids = routes.reshape(-1)
    onehot = (flat_ids[:, None] == jnp.arange(experts, dtype=jnp.int32)[None, :]).astype(jnp.int32)
    slot_rank = jnp.sum((jnp.cumsum(onehot, axis=0) - onehot) * onehot, axis=-1)
    destination = (flat_ids * capacity + slot_rank).reshape(tok_rows, 2)
    slot_ids = jnp.arange(experts * capacity, dtype=jnp.int32)
    hits = slot_ids[:, None, None] == destination[None, :, :]
    dispatch = jnp.any(hits, axis=-1).astype(jnp.bfloat16)
    outgoing = jnp.dot(dispatch, normed, preferred_element_type=jnp.float32).astype(jnp.bfloat16)
    outgoing = outgoing.reshape(fs_count, EXP_DEV, capacity, tokens.shape[1])
    arrived = lax.all_to_all(outgoing, "fs", split_axis=0, concat_axis=0, tiled=True)
    gate = jnp.einsum("sjnd,jdf->sjnf", arrived, gate_out, preferred_element_type=jnp.float32)
    upper = jnp.einsum("sjnd,jdf->sjnf", arrived, up_out, preferred_element_type=jnp.float32)
    hidden = (jax.nn.silu(gate) * upper).astype(jnp.bfloat16)
    partial_value = jnp.einsum(
        "sjnf,jdf->sjnd", hidden, down_out, preferred_element_type=jnp.float32
    )
    rounded = lax.optimization_barrier(partial_value.astype(jnp.bfloat16))
    summed = lax.psum_scatter(
        rounded.astype(jnp.float32).astype(jnp.bfloat16), "tp", scatter_dimension=3, tiled=True
    )
    back_home = lax.all_to_all(summed, "fs", split_axis=0, concat_axis=0, tiled=True)
    features = back_home.shape[-1]
    flat_back = back_home.reshape(experts * capacity, features).astype(jnp.float32)
    first = jnp.where(slot_ids[None, :] == destination[:, 0:1], route_weight[:, 0:1], 0.0)
    second = jnp.where(slot_ids[None, :] == destination[:, 1:2], route_weight[:, 1:2], 0.0)
    combine_map = first + second
    mixed = jnp.dot(
        combine_map, flat_back, precision=lax.Precision.HIGHEST, preferred_element_type=jnp.float32
    ).astype(jnp.bfloat16)
    return (gate_out, up_out, down_out, mixed)


def solution(mesh):
    in_specs = (
        P(("gr", "fs"), None),
        P(("gr", "fs"), None),
        P(("gr", "fs"), None),
        P(("gr", "fs")),
        P(None, ("gr", "fs"), "tp"),
        P(None, ("gr", "fs"), "tp"),
        P(None, ("gr", "fs"), "tp"),
    )
    out_specs = (
        P("fs", None, "tp"),
        P("fs", None, "tp"),
        P("fs", None, "tp"),
        P(("gr", "fs"), "tp"),
    )
    ng, nz, nt = mesh.shape["gr"], mesh.shape["fs"], mesh.shape["tp"]
    small = ng == 2 and nt == 4 and nz == 4
    work = functools.partial(fused, ng, nz, nt) if small else body
    return jax.shard_map(work, mesh=mesh, in_specs=in_specs, out_specs=out_specs, check_vma=False)
```

```python
import functools
import jax
import jax.numpy as jnp
from jax import lax
from jax.experimental import pallas as pl
from jax.experimental.pallas import tpu as pltpu
from jax.sharding import PartitionSpec as P

MESH = pl.DeviceIdType.MESH
VMEM_LIMIT = 50 * 1024 * 1024
EPSILON = 1e-05
BLOCKS = 4
LAG = 4


def kernel(ng, nz, nt, tok_in, routes, rweight, gain, gw, uw, dw, gout, uout, dout, mixed,
           tok, packed, hid, part, crx, yrx, full, stage, raw, ret, rly, wsend, wrecv, wcol, gcol, before, pick, spread,
           ld, ts, tr, fs_s, fr, gs, gr, zs, zr, xs, xr, cs, cr, ys, yr, hs, hr, rs, rr):
    g, z, t = lax.axis_index("gr"), lax.axis_index("fs"), lax.axis_index("tp")
    core, y = lax.rem(t, 2), lax.div(t, 2)
    rows, d = tok_in.shape
    quarter = d // nt
    chunk, width = gw.shape[1], gw.shape[2]
    half = chunk // 2
    cap = packed.shape[1]
    chunks = ng * nz
    per_owner = chunks // nt
    nb = BLOCKS
    blk = width // nb
    outs = (gout, uout)
    mate, over = y * 2 + 1 - core, (1 - y) * 2 + core
    inner = jnp.logical_and(z > 0, z < nz - 1)
    side = lax.div(z, 2)
    pair = z + 1 - 2 * lax.rem(z, 2)
    far = (3 * (1 - side), 2 - side)
    order = (far[0], far[1], pair, z)
    odd = lax.rem(z, 2)
    k_near = 3 - 2 * odd
    near_to = 4 - k_near
    k_mid = jnp.where(inner, near_to, 2)
    k_far = jnp.where(inner, 2, near_to)

    def to(k):
        return lax.rem(z + k, nz)

    def frm(k):
        return lax.rem(z + nz - k, nz)

    def rdma(src, dst, ss, rsem, dev):
        return pltpu.make_async_remote_copy(
            src_ref=src, dst_ref=dst, send_sem=ss, recv_sem=rsem, device_id=dev, device_id_type=MESH
        )

    def row0(group, zsrc):
        return pl.multiple_of((group * nz + zsrc) * chunk, chunk)

    def cols(b):
        return pl.ds(pl.multiple_of(b * blk, blk), blk)

    def qcols(q):
        return pl.ds(pl.multiple_of(q * quarter, quarter), quarter)

    def piece(m, b, group, zsrc):
        return outs[m].at[pl.ds(row0(group, zsrc), chunk), cols(b)]

    def dpiece(m, group, zsrc):
        return dout.at[pl.ds(pl.multiple_of(row0(group, zsrc) + m * half, half), half), :]

    def z_copy(m, b, k):
        return rdma(stage.at[m, to(k), :, cols(b)], piece(m, b, g, z), zs.at[m, b, k], zr.at[m, b, k], {"fs": to(k)})

    def zd_copy(m, k):
        return rdma(dw.at[to(k), pl.ds(m * half, half), :], dpiece(m, g, z), zs.at[m, nb, k], zr.at[m, nb, k], {"fs": to(k)})

    def x_own(m, b):
        return rdma(stage.at[m, z, :, cols(b)], piece(m, b, g, z), xs.at[m, b, 0], xr.at[m, b, 0], {"gr": 1 - g})

    def xd_own(m):
        return rdma(dw.at[z, pl.ds(m * half, half), :], dpiece(m, g, z), xs.at[m, nb, 0], xr.at[m, nb, 0], {"gr": 1 - g})

    def relay(ref, m, b, k):
        return rdma(ref, ref, xs.at[m, b, k], xr.at[m, b, k], {"gr": 1 - g})

    def z_arrive(ref, m, b, k):
        rdma(ref, ref, zs.at[m, b, k], zr.at[m, b, k], {"fs": to(k)}).wait_recv()

    def z_take(b, k):
        for m in range(2):
            ref = piece(m, b, g, frm(k))
            z_arrive(ref, m, b, k)
            relay(ref, m, b, k).start()

    def zd_take(k, ms=(0, 1)):
        for m in ms:
            ref = dpiece(m, g, frm(k))
            z_arrive(ref, m, nb, k)
            relay(ref, m, nb, k).start()

    def order_of(j):
        return jnp.where(j == 0, far[0], jnp.where(j == 1, far[1], jnp.where(j == 2, pair, z)))

    def k_of(s):
        return jnp.where(s == 0, 0, jnp.where(s == 1, k_near, jnp.where(s == 2, k_far, k_mid)))

    def z_cross(b, ms=(0, 1)):
        for m in ms:
            for k in (2, k_near):
                z_copy(m, b, k).start()

    def z_side(b):
        for m in range(2):
            z_copy(m, b, near_to).start()

    def z_down_side():
        for m in range(2):
            zd_copy(m, near_to).start()

    def z_down_cross():
        for m in range(2):
            for k in (2, k_near):
                zd_copy(m, k).start()

    load_tok = pltpu.make_async_copy(tok_in, raw, ld.at[0])
    loads = [pltpu.make_async_copy(src, stage.at[m], ld.at[1 + m]) for m, src in enumerate((gw, uw))]
    own_rows = pl.ds(row0(g, z), chunk)
    own_down = pltpu.make_async_copy(dw.at[z], dout.at[own_rows, :], ld.at[3])
    load_tok.start()
    for c in loads:
        c.start()
    own_down.start()

    barrier = pltpu.get_barrier_semaphore()
    for k in range(1, nz):
        pl.semaphore_signal(barrier, inc=1, device_id={"fs": to(k)}, device_id_type=MESH)
    for who in (mate, over):
        pl.semaphore_signal(barrier, inc=1, device_id={"tp": who}, device_id_type=MESH)
    pl.semaphore_signal(barrier, inc=1, device_id={"gr": 1 - g}, device_id_type=MESH)

    step = 64

    def norm():
        load_tok.wait()

        @pl.loop(0, rows // step)
        def _(i):
            at = pl.ds(pl.multiple_of(i * step, step), step)
            v = raw[at, :].astype(jnp.float32)
            scale = lax.rsqrt(jnp.mean(v * v, axis=-1, keepdims=True) + EPSILON)
            tok[z, at, :] = (v * scale).astype(jnp.bfloat16)

    norm()
    pl.semaphore_wait(barrier, nz - 1 + 3)

    guarded = []

    def guard(flag, c):
        @pl.when(flag)
        def _():
            c.start()
        guarded.append((flag, c))

    def hop(way, h, src):
        ref = tok.at[src, :, qcols(t)]
        nxt = lax.rem(z + way + nz, nz)
        return rdma(ref, ref, ts.at[(way + 1) // 2, h], tr.at[src], {"fs": nxt})

    right, left = z + 1 < nz, z >= 1
    for e in range(nz):
        wsend[e] = (
            jnp.where(routes[0:1, :] == e, rweight[0:1, :], 0.0)
            + jnp.where(routes[1:2, :] == e, rweight[1:2, :], 0.0)
        )
    wrecv[z] = wsend[z]
    for k in range(1, nz):
        rdma(wsend.at[to(k)], wrecv.at[z], gs.at[k], gr.at[k], {"fs": to(k)}).start()
    guard(right, hop(1, 0, z))
    guard(left, hop(-1, 0, z))
    for m in range(2):
        xd_own(m).start()

    def scaleall():
        gcol[...] = jnp.transpose(jnp.broadcast_to(gain[...], (128, chunk)))
        for c in loads:
            c.wait()

        @pl.loop(0, nz * (chunk // step))
        def _(i):
            e = i // (chunk // step)
            at = pl.ds(pl.multiple_of(lax.rem(i, chunk // step) * step, step), step)
            factor = jnp.concatenate([gcol[at, :]] * (width // 128), axis=1)
            for m in range(2):
                stage[m, e, at, :] = (stage[m, e, at, :].astype(jnp.float32) * factor).astype(jnp.bfloat16)

    scaleall()
    @pl.when(jnp.logical_not(inner))
    def _():
        pl.loop(0, nb)(z_side)
        pl.loop(0, nb)(z_cross)

    @pl.when(inner)
    def _():
        z_side(0)
        z_cross(0, (0,))

    for b in range(nb):
        for m in range(2):
            x_own(m, b).start()

    for m in range(2):
        outs[m][own_rows, :] = stage[m, z]
    before[...] = jnp.where(
        lax.broadcasted_iota(jnp.int32, (rows, rows), 0) < lax.broadcasted_iota(jnp.int32, (rows, rows), 1), 1.0, 0.0
    ).astype(jnp.bfloat16)

    def hops(h):
        for way in (1, -1):
            src = lax.rem(z - way * h + nz, nz)
            valid = z >= h if way == 1 else z + h < nz
            more = right if way == 1 else left
            ref = tok.at[src, :, qcols(t)]

            @pl.when(valid)
            def _(ref=ref, src=src):
                rdma(ref, ref, ts.at[0, 0], tr.at[src], {"fs": lax.rem(z + 1, nz)}).wait_recv()
            guard(jnp.logical_and(valid, more), hop(way, h, src))
            guard(valid, rdma(ref, ref, fs_s.at[1, src], fr.at[1, src], {"tp": over}))
            guard(valid, rdma(ref, ref, fs_s.at[0, src], fr.at[0, src], {"tp": mate}))

    def token_quarter(lane, src, q):
        ref = tok.at[src, :, qcols(q)]
        return rdma(ref, ref, fs_s.at[lane, src], fr.at[lane, src], {"tp": mate})

    def forward(s):
        src = frm(k_of(s))
        token_quarter(1, src, over).wait_recv()
        token_quarter(2, src, over).start()

    def tok_wait(src, s):
        token_quarter(0, src, mate).wait_recv()
        token_quarter(2, src, (1 - y) * 2 + 1 - core).wait_recv()
        rdma(wrecv.at[src], wrecv.at[src], gs.at[s], gr.at[s], {"fs": to(s)}).wait_recv()

    def prepare(s):
        src = frm(k_of(s))

        @pl.when(s >= 1)
        def _():
            tok_wait(src, k_of(s))
        weight = wrecv[src]
        chosen = weight != 0.0
        marks = jnp.broadcast_to(jnp.where(chosen, 1.0, 0.0), (16, rows)).astype(jnp.bfloat16)
        rank = jnp.dot(marks, before[...], preferred_element_type=jnp.float32)[0:1]
        key = jnp.where(chosen, rank, -1.0)
        match = key == lax.broadcasted_iota(jnp.int32, (cap, rows), 0).astype(jnp.float32)
        own_weight = jnp.sum(jnp.where(match, weight, 0.0), axis=1, keepdims=True)
        wcol[src] = jnp.broadcast_to(own_weight, (cap, 128))
        pick[...] = jnp.where(match, 1.0, 0.0).astype(jnp.bfloat16)
        column = jnp.transpose(jnp.broadcast_to(key, (128, rows)))
        lane = lax.broadcasted_iota(jnp.int32, (rows, 128), 1).astype(jnp.float32)
        for v in range(cap // 128):
            spread[src, :, v * 128:(v + 1) * 128] = jnp.where(column == lane + v * 128.0, 1.0, 0.0).astype(jnp.bfloat16)

        @pl.loop(0, nt)
        def _(q):
            packed[src, :, qcols(q)] = jnp.dot(
                pick[...], tok[src, :, qcols(q)], preferred_element_type=jnp.float32
            ).astype(jnp.bfloat16)

    def take_near(lo, hi):
        @pl.loop(lo, hi)
        def _(b):
            z_take(b, k_near)

    ends = jnp.logical_not(inner)
    hops(1)

    @pl.when(inner)
    def _():
        z_cross(0, (1,))
        take_near(0, nb // 2)

    @pl.when(ends)
    def _():
        z_take(0, k_near)
    hops(2)

    @pl.when(inner)
    def _():
        pl.loop(1, nb)(z_side)
        pl.loop(1, nb)(z_cross)
        z_down_side()
        z_down_cross()
        take_near(nb // 2, nb)

    @pl.when(ends)
    def _():
        z_take(0, k_far)
    for h in range(3, nz):
        hops(h)
    for s in (1, 3):
        forward(s)

    @pl.when(inner)
    def _():
        forward(2)
    pl.loop(0, 2)(prepare)

    @pl.loop(0, nb)
    def _(b):
        @pl.when(jnp.logical_or(inner, b >= 1))
        def _():
            z_take(b, k_far)

        @pl.when(jnp.logical_and(ends, lax.rem(b, 2) == 1))
        def _():
            z_take(b // 2 + 1, k_near)

        @pl.when(b == 0)
        def _():
            prepare(3)

            @pl.when(ends)
            def _():
                forward(2)

        @pl.when(b == 1)
        def _():
            prepare(2)

        @pl.when(b == nb // 2)
        def _():
            z_take(0, k_mid)

    def x_wait(b):
        @pl.loop(0, nz)
        def _(kk):
            for m in range(2):
                ref = piece(m, b, 1 - g, frm(kk))
                rdma(ref, ref, xs.at[m, b, kk], xr.at[m, b, kk], {"gr": 1 - g}).wait_recv()

    def hidden(b, src):
        a = packed[src]
        gate = jnp.dot(a, gout[:, cols(b)], preferred_element_type=jnp.float32)
        upper = jnp.dot(a, uout[:, cols(b)], preferred_element_type=jnp.float32)
        weight = jnp.concatenate([wcol[src]] * (blk // 128), axis=1)
        hid[src, :, cols(b)] = (gate / (1.0 + jnp.exp(-gate)) * upper * weight).astype(jnp.bfloat16)

    @pl.loop(nz, (nb + 1) * nz)
    def _(i):
        b, s = i // nz, lax.rem(i, nz)
        src = frm(k_of(s))

        @pl.when(jnp.logical_and(s == 0, b < nb))
        def _():
            z_take(b, k_mid)

        @pl.when(jnp.logical_and(jnp.logical_not(inner), jnp.logical_and(s == 1, b < nb - nb // 2)))
        def _():
            z_take(b + nb // 2, k_near)

        @pl.when(jnp.logical_and(jnp.logical_not(inner), i == (nb - 2) * nz))
        def _():
            z_down_side()

        @pl.when(jnp.logical_and(jnp.logical_not(inner), i == nb * nz))
        def _():
            z_down_cross()
            zd_take(k_near)

        @pl.when(s == 0)
        def _():
            x_wait(b - 1)

        hidden(b - 1, src)

    own_down.wait()

    def chunk_of(i):
        k, other = k_of(i // 2), lax.rem(i, 2)
        group = g + other * (1 - 2 * g)
        c = group * nz + frm(k)
        owner = c // per_owner
        return k, other, c, owner, lax.rem(owner, 2), owner // 2, lax.rem(c, per_owner)

    def cut(ref, h):
        return ref if h is None else ref.at[:, pl.ds(h * half, half)]

    def slot_of(i, h):
        return i + 2 if h == 1 else i

    def give(i, j, h):
        k, other, c, owner, par, yo, cc = chunk_of(i)
        b, si = order_of(j), slot_of(i, h)
        src, dst = cut(part.at[c, b], h), cut(crx.at[yo * per_owner + cc, b], h)
        return rdma(src, dst, cs.at[si, j], cr.at[si, j], {"tp": mate})

    def up(i, j, h):
        k, other, c, owner, par, yo, cc = chunk_of(i)
        si = slot_of(i, h)
        src, dst = cut(part.at[c, order[j]], h), cut(yrx.at[cc, order[j]], h)
        return rdma(src, dst, ys.at[si, j], yr.at[si, j], {"tp": over})

    def near(cc, j, h):
        second = 1 if h == 1 else 0
        dst = rly.at[j, cc] if j < 2 else ret.at[0, cc]
        landed = hr.at[j, cc, second if j < 2 else 0]
        return rdma(cut(full.at[cc, order[j]], h), cut(dst, h), hs.at[j, cc, second], landed, {"fs": pair})

    def cross(cc, j, h):
        second = 1 if h == 1 else 0
        src, dst = cut(full.at[cc, order[j]], h), cut(ret.at[1, cc], h)
        return rdma(src, dst, rs.at[j, cc, second], rr.at[cc], {"fs": order[j]})

    def x_down_wait(k, ms):
        for m in ms:
            ref = dpiece(m, 1 - g, frm(k))
            rdma(ref, ref, xs.at[m, nb, k], xr.at[m, nb, k], {"gr": 1 - g}).wait_recv()

    def stage_a(i):
        k, other, c, owner, par, yo, cc = chunk_of(i)

        @pl.when(other == 1)
        def _():
            x_down_wait(k, range(2))
        mine = pl.ds(pl.multiple_of(c * chunk, chunk), chunk)

        @pl.loop(0, nz)
        def _(j):
            b = order_of(j)
            part[c, b] = lax.dot_general(
                hid[b], dout[mine, :], (((1,), (1,)), ((), ())), preferred_element_type=jnp.float32
            ).astype(jnp.bfloat16)

            @pl.when(par != core)
            def _():
                give(i, j, None).start()

    def halves_a(i, h):
        k, other, c, owner, par, yo, cc = chunk_of(i)
        c2 = chunk_of(i + 1)[2]
        x_down_wait(k, (h,))
        mine = [pl.ds(pl.multiple_of(v * chunk + h * half, half), half) for v in (c, c2)]

        @pl.loop(0, nz)
        def _(j):
            b = order_of(j)
            both = lax.dot_general(
                hid[b], jnp.concatenate([dout[v, :] for v in mine], axis=0), (((1,), (1,)), ((), ())),
                preferred_element_type=jnp.float32,
            ).astype(jnp.bfloat16)
            cut(part.at[c, b], h)[...] = both[:, :half]
            cut(part.at[c2, b], h)[...] = both[:, half:]

            @pl.when(par != core)
            def _():
                give(i, j, h).start()
                give(i + 1, j, h).start()

    def add(target, h, ref):
        mine = cut(target, h)
        mine[...] = (mine[...].astype(jnp.float32) + ref[...].astype(jnp.float32)).astype(jnp.bfloat16)

    def stage_b(i, h=None):
        k, other, c, owner, par, yo, cc = chunk_of(i)
        si = slot_of(i, h)

        @pl.when(par == core)
        def _():
            for j in range(nz):
                b = order[j]
                ref = cut(crx.at[yo * per_owner + cc, b], h)
                rdma(ref, ref, cs.at[si, j], cr.at[si, j], {"tp": mate}).wait_recv()
                add(part.at[c, b], h, ref)

                @pl.when(yo != y)
                def _(j=j):
                    up(i, j, h).start()

    def stage_c(i, h=None):
        k, other, c, owner, par, yo, cc = chunk_of(i)
        si = slot_of(i, h)

        @pl.when(owner == t)
        def _():
            for j in range(nz):
                b = order[j]
                ref = cut(yrx.at[cc, b], h)
                rdma(ref, ref, ys.at[si, j], yr.at[si, j], {"tp": over}).wait_recv()
                total = cut(part.at[c, b], h)[...].astype(jnp.float32) + ref[...].astype(jnp.float32)
                cut(full.at[cc, b], h)[...] = jnp.dot(
                    spread[b], total.astype(jnp.bfloat16), preferred_element_type=jnp.float32
                ).astype(jnp.bfloat16)
                if j < 2:
                    @pl.when(jnp.logical_not(inner))
                    def _(j=j):
                        near(cc, j, h).start()
                elif j == 2:
                    near(cc, j, h).start()

    def cross_phase(cc, h=None):
        for j in range(2):
            ref = cut(rly.at[j, cc], h)
            rdma(ref, ref, hs.at[j, cc, 0], hr.at[j, cc, 1 if h == 1 else 0], {"fs": pair}).wait_recv()
            add(full.at[cc, order[j]], h, ref)
            cross(cc, j, h).start()

    n = chunks
    early = jnp.logical_and(inner, side == core)
    late = jnp.logical_and(inner, side != core)
    cc_far = lax.rem(frm(k_far), 2)

    @pl.when(inner)
    def _():
        zd_take(k_near)

    @pl.loop(0, n - 2)
    def _(i):
        @pl.when(i == 2)
        def _():
            zd_take(k_far, (0,))

        @pl.when(i == 4)
        def _():
            zd_take(k_far, (1,))
            pl.loop(0, 2)(stage_c)

        stage_a(i)
        stage_b(i)

    zd_take(k_mid, (0,))
    pl.loop(2, 4)(stage_c)

    def last(h):
        halves_a(n - 2, h)

        @pl.loop(n - 2, n)
        def _(i):
            stage_b(i, h)

    last(0)
    zd_take(k_mid, (1,))

    @pl.when(early)
    def _():
        pl.loop(0, per_owner)(cross_phase)
    pl.loop(n - 4, n - 2)(stage_c)

    @pl.when(late)
    def _():
        cross_phase(cc_far)
    last(1)
    for h in range(2):
        @pl.loop(n - 2, n)
        def _(i, h=h):
            stage_c(i, h)

        @pl.when(late)
        def _(h=h):
            cross_phase(1 - cc_far, h)

    def final():
        for cc in range(per_owner):
            direct, crossed = ret.at[0, cc], ret.at[1, cc]
            rdma(direct, direct, hs.at[2, cc, 0], hr.at[2, cc, 0], {"fs": pair}).wait_recv()
            rdma(crossed, crossed, rs.at[0, cc, 0], rr.at[cc], {"fs": pair}).wait_recv()
            mixed[:, cc * chunk:(cc + 1) * chunk] = (
                full[cc, z].astype(jnp.float32)
                + ret[0, cc].astype(jnp.float32)
                + ret[1, cc].astype(jnp.float32)
            ).astype(jnp.bfloat16)

    final()

    def send_waits():
        @pl.loop(1, nz)
        def _(k):
            rdma(wsend.at[to(k)], wrecv.at[z], gs.at[k], gr.at[k], {"fs": to(k)}).wait_send()
            for m in range(2):
                zd_copy(m, k).wait_send()
                relay(dpiece(m, g, frm(k)), m, nb, k).wait_send()
            token_quarter(2, frm(k), over).wait_send()

            @pl.loop(0, nb)
            def _(b):
                for m in range(2):
                    z_copy(m, b, k).wait_send()
                    relay(piece(m, b, g, frm(k)), m, b, k).wait_send()

        for m in range(2):
            xd_own(m).wait_send()

            @pl.loop(0, nb)
            def _(b):
                x_own(m, b).wait_send()

        for flag, c in guarded:
            @pl.when(flag)
            def _(c=c):
                c.wait_send()

        def sent(i, h):
            k, other, c, owner, par, yo, cc = chunk_of(i)

            @pl.when(par != core)
            def _():
                for j in range(nz):
                    give(i, j, h).wait_send()

            @pl.when(jnp.logical_and(par == core, yo != y))
            def _():
                for j in range(nz):
                    up(i, j, h).wait_send()

        def returned(cc, h):
            near(cc, 2, h).wait_send()
            for j in range(2):
                @pl.when(inner)
                def _(j=j):
                    cross(cc, j, h).wait_send()

                @pl.when(jnp.logical_not(inner))
                def _(j=j):
                    near(cc, j, h).wait_send()

        @pl.loop(0, n - 2)
        def _(i):
            sent(i, None)
        for h in range(2):
            @pl.loop(n - 2, n)
            def _(i, h=h):
                sent(i, h)
        returned(cc_far, None)

        @pl.when(side == core)
        def _():
            returned(1 - cc_far, None)

        @pl.when(side != core)
        def _():
            for h in range(2):
                returned(1 - cc_far, h)

    send_waits()


def store(gate, upper, down, mixed, gate_out, up_out, down_out, mixed_out, sem):
    copies = [
        pltpu.make_async_copy(gate, gate_out.at[0], sem.at[0]),
        pltpu.make_async_copy(upper, up_out.at[0], sem.at[1]),
        pltpu.make_async_copy(down, down_out.at[0], sem.at[2]),
        pltpu.make_async_copy(mixed, mixed_out, sem.at[3]),
    ]
    for c in copies:
        c.start()
    for c in copies:
        c.wait()


def fused(ng, nz, nt, tokens, routes, route_weight, gain, w_gate, w_up, w_down):
    rows, d = tokens.shape
    quarter = d // nt
    experts, chunk, width = w_gate.shape
    chunks = ng * nz
    per_owner = chunks // nt
    cap = 3 * rows // experts
    bf, f32 = jnp.bfloat16, jnp.float32
    dma = pltpu.SemaphoreType.DMA
    full = pltpu.VMEM((d, width), bf)
    vmem = pl.BlockSpec(memory_space=pltpu.VMEM)
    anywhere = pl.BlockSpec(memory_space=pl.ANY)
    results = pl.pallas_call(
        functools.partial(kernel, ng, nz, nt),
        out_shape=(full, full, full, pltpu.VMEM((rows, quarter), bf)),
        in_specs=[anywhere, vmem, vmem, vmem, anywhere, anywhere, anywhere],
        out_specs=(vmem,) * 4,
        scratch_shapes=[
            pltpu.VMEM((nz, rows, d), bf),
            pltpu.VMEM((nz, cap, d), bf),
            pltpu.VMEM((nz, cap, width), bf),
            pltpu.VMEM((chunks, nz, cap, chunk), bf),
            pltpu.VMEM((chunks // 2, nz, cap, chunk), bf),
            pltpu.VMEM((per_owner, nz, cap, chunk), bf),
            pltpu.VMEM((per_owner, nz, rows, chunk), bf),
            pltpu.VMEM((2, nz, chunk, width), bf),
            pltpu.VMEM((rows, d), bf),
            pltpu.VMEM((2, per_owner, rows, chunk), bf),
            pltpu.VMEM((2, per_owner, rows, chunk), bf),
            pltpu.VMEM((nz, 1, rows), f32),
            pltpu.VMEM((nz, 1, rows), f32),
            pltpu.VMEM((nz, cap, 128), f32),
            pltpu.VMEM((chunk, 128), f32),
            pltpu.VMEM((rows, rows), bf),
            pltpu.VMEM((cap, rows), bf),
            pltpu.VMEM((nz, rows, cap), bf),
            dma((4,)),
            dma((2, nz)), dma((nz,)),
            dma((3, nz)), dma((3, nz)),
            dma((nz,)), dma((nz,)),
            dma((2, BLOCKS + 1, nz)), dma((2, BLOCKS + 1, nz)),
            dma((2, BLOCKS + 1, nz)), dma((2, BLOCKS + 1, nz)),
            dma((chunks + 2, nz)), dma((chunks + 2, nz)),
            dma((chunks + 2, nz)), dma((chunks + 2, nz)),
            dma((3, per_owner, 2)), dma((3, per_owner, 2)),
            dma((2, per_owner, 2)), dma((per_owner,)),
        ],
        compiler_params=pltpu.CompilerParams(
            collective_id=0, has_side_effects=True, vmem_limit_bytes=VMEM_LIMIT
        ),
    )(tokens, routes.T, route_weight.T, gain.reshape(1, chunk), w_gate, w_up, w_down)
    whole = jax.ShapeDtypeStruct((1, d, width), bf)
    return pl.pallas_call(
        store,
        out_shape=(whole, whole, whole, jax.ShapeDtypeStruct((rows, quarter), bf)),
        in_specs=[vmem] * 4,
        out_specs=(anywhere,) * 4,
        scratch_shapes=[dma((4,))],
        compiler_params=pltpu.CompilerParams(vmem_limit_bytes=4 * 1024 * 1024),
    )(*results)

EXP_DEV = 1


def body(tokens, routes, route_weight, gain, w_gate, w_up, w_down):
    scaling = gain[None, :, None]
    gate_local = (w_gate * scaling).astype(jnp.bfloat16)
    up_local = (w_up * scaling).astype(jnp.bfloat16)
    gate_mine, up_mine, down_mine = (
        lax.all_to_all(gate_local, "fs", split_axis=0, concat_axis=1, tiled=True),
        lax.all_to_all(up_local, "fs", split_axis=0, concat_axis=1, tiled=True),
        lax.all_to_all(w_down, "fs", split_axis=0, concat_axis=1, tiled=True),
    )
    gate_out, up_out, down_out = (
        lax.all_gather(gate_mine, "gr", axis=1, tiled=True),
        lax.all_gather(up_mine, "gr", axis=1, tiled=True),
        lax.all_gather(down_mine, "gr", axis=1, tiled=True),
    )
    fs_count = lax.axis_size("fs")
    experts = EXP_DEV * fs_count
    tok_rows = tokens.shape[0]
    capacity = 3 * tok_rows // experts
    float_rows = tokens.astype(jnp.float32)
    normed = (
        float_rows * lax.rsqrt(jnp.mean(float_rows * float_rows, axis=-1, keepdims=True) + EPSILON)
    ).astype(jnp.bfloat16)
    flat_ids = routes.reshape(-1)
    onehot = (flat_ids[:, None] == jnp.arange(experts, dtype=jnp.int32)[None, :]).astype(jnp.int32)
    slot_rank = jnp.sum((jnp.cumsum(onehot, axis=0) - onehot) * onehot, axis=-1)
    destination = (flat_ids * capacity + slot_rank).reshape(tok_rows, 2)
    slot_ids = jnp.arange(experts * capacity, dtype=jnp.int32)
    hits = slot_ids[:, None, None] == destination[None, :, :]
    dispatch = jnp.any(hits, axis=-1).astype(jnp.bfloat16)
    outgoing = jnp.dot(dispatch, normed, preferred_element_type=jnp.float32).astype(jnp.bfloat16)
    outgoing = outgoing.reshape(fs_count, EXP_DEV, capacity, tokens.shape[1])
    arrived = lax.all_to_all(outgoing, "fs", split_axis=0, concat_axis=0, tiled=True)
    gate = jnp.einsum("sjnd,jdf->sjnf", arrived, gate_out, preferred_element_type=jnp.float32)
    upper = jnp.einsum("sjnd,jdf->sjnf", arrived, up_out, preferred_element_type=jnp.float32)
    hidden = (jax.nn.silu(gate) * upper).astype(jnp.bfloat16)
    partial_value = jnp.einsum(
        "sjnf,jdf->sjnd", hidden, down_out, preferred_element_type=jnp.float32
    )
    rounded = lax.optimization_barrier(partial_value.astype(jnp.bfloat16))
    summed = lax.psum_scatter(
        rounded.astype(jnp.float32).astype(jnp.bfloat16), "tp", scatter_dimension=3, tiled=True
    )
    back_home = lax.all_to_all(summed, "fs", split_axis=0, concat_axis=0, tiled=True)
    features = back_home.shape[-1]
    flat_back = back_home.reshape(experts * capacity, features).astype(jnp.float32)
    first = jnp.where(slot_ids[None, :] == destination[:, 0:1], route_weight[:, 0:1], 0.0)
    second = jnp.where(slot_ids[None, :] == destination[:, 1:2], route_weight[:, 1:2], 0.0)
    combine_map = first + second
    mixed = jnp.dot(
        combine_map, flat_back, precision=lax.Precision.HIGHEST, preferred_element_type=jnp.float32
    ).astype(jnp.bfloat16)
    return (gate_out, up_out, down_out, mixed)


def solution(mesh):
    in_specs = (
        P(("gr", "fs"), None),
        P(("gr", "fs"), None),
        P(("gr", "fs"), None),
        P(("gr", "fs")),
        P(None, ("gr", "fs"), "tp"),
        P(None, ("gr", "fs"), "tp"),
        P(None, ("gr", "fs"), "tp"),
    )
    out_specs = (
        P("fs", None, "tp"),
        P("fs", None, "tp"),
        P("fs", None, "tp"),
        P(("gr", "fs"), "tp"),
    )
    ng, nz, nt = mesh.shape["gr"], mesh.shape["fs"], mesh.shape["tp"]
    small = ng == 2 and nt == 4 and nz == 4
    work = functools.partial(fused, ng, nz, nt) if small else body
    return jax.shard_map(work, mesh=mesh, in_specs=in_specs, out_specs=out_specs, check_vma=False)
```

```python
import functools
import jax
import jax.numpy as jnp
from jax import lax
from jax.experimental import pallas as pl
from jax.experimental.pallas import tpu as pltpu
from jax.sharding import PartitionSpec as P

MESH = pl.DeviceIdType.MESH
VMEM_LIMIT = 50 * 1024 * 1024
EPSILON = 1e-05
BLOCKS = 4
LAG = 4


def kernel(ng, nz, nt, tok_in, routes, rweight, gain, gw, uw, dw, gout, uout, dout, mixed,
           tok, packed, hid, part, crx, yrx, full, stage, raw, ret, rly, wsend, wrecv, wcol, gcol, before, pick, spread,
           ld, ts, tr, fs_s, fr, gs, gr, zs, zr, xs, xr, cs, cr, ys, yr, hs, hr, rs, rr):
    g, z, t = lax.axis_index("gr"), lax.axis_index("fs"), lax.axis_index("tp")
    core, y = lax.rem(t, 2), lax.div(t, 2)
    rows, d = tok_in.shape
    quarter = d // nt
    chunk, width = gw.shape[1], gw.shape[2]
    half = chunk // 2
    cap = packed.shape[1]
    chunks = ng * nz
    per_owner = chunks // nt
    nb = BLOCKS
    blk = width // nb
    outs = (gout, uout)
    mate, over = y * 2 + 1 - core, (1 - y) * 2 + core
    inner = jnp.logical_and(z > 0, z < nz - 1)
    side = lax.div(z, 2)
    pair = z + 1 - 2 * lax.rem(z, 2)
    far = (3 * (1 - side), 2 - side)
    order = (far[0], far[1], pair, z)
    odd = lax.rem(z, 2)
    k_near = 3 - 2 * odd
    near_to = 4 - k_near
    k_mid = jnp.where(inner, near_to, 2)
    k_far = jnp.where(inner, 2, near_to)

    def to(k):
        return lax.rem(z + k, nz)

    def frm(k):
        return lax.rem(z + nz - k, nz)

    def rdma(src, dst, ss, rsem, dev):
        return pltpu.make_async_remote_copy(
            src_ref=src, dst_ref=dst, send_sem=ss, recv_sem=rsem, device_id=dev, device_id_type=MESH
        )

    def row0(group, zsrc):
        return pl.multiple_of((group * nz + zsrc) * chunk, chunk)

    def cols(b):
        return pl.ds(pl.multiple_of(b * blk, blk), blk)

    def qcols(q):
        return pl.ds(pl.multiple_of(q * quarter, quarter), quarter)

    def piece(m, b, group, zsrc):
        return outs[m].at[pl.ds(row0(group, zsrc), chunk), cols(b)]

    def dpiece(m, group, zsrc):
        return dout.at[pl.ds(pl.multiple_of(row0(group, zsrc) + m * half, half), half), :]

    def z_copy(m, b, k):
        return rdma(stage.at[m, to(k), :, cols(b)], piece(m, b, g, z), zs.at[m, b, k], zr.at[m, b, k], {"fs": to(k)})

    def zd_copy(m, k):
        return rdma(dw.at[to(k), pl.ds(m * half, half), :], dpiece(m, g, z), zs.at[m, nb, k], zr.at[m, nb, k], {"fs": to(k)})

    def x_own(m, b):
        return rdma(stage.at[m, z, :, cols(b)], piece(m, b, g, z), xs.at[m, b, 0], xr.at[m, b, 0], {"gr": 1 - g})

    def xd_own(m):
        return rdma(dw.at[z, pl.ds(m * half, half), :], dpiece(m, g, z), xs.at[m, nb, 0], xr.at[m, nb, 0], {"gr": 1 - g})

    def relay(ref, m, b, k):
        return rdma(ref, ref, xs.at[m, b, k], xr.at[m, b, k], {"gr": 1 - g})

    def z_arrive(ref, m, b, k):
        rdma(ref, ref, zs.at[m, b, k], zr.at[m, b, k], {"fs": to(k)}).wait_recv()

    def z_take(b, k):
        for m in range(2):
            ref = piece(m, b, g, frm(k))
            z_arrive(ref, m, b, k)
            relay(ref, m, b, k).start()

    def zd_take(k, ms=(0, 1)):
        for m in ms:
            ref = dpiece(m, g, frm(k))
            z_arrive(ref, m, nb, k)
            relay(ref, m, nb, k).start()

    def order_of(j):
        return jnp.where(j == 0, far[0], jnp.where(j == 1, far[1], jnp.where(j == 2, pair, z)))

    def k_of(s):
        return jnp.where(s == 0, 0, jnp.where(s == 1, k_near, jnp.where(s == 2, k_far, k_mid)))

    def z_cross(b, ms=(0, 1)):
        for m in ms:
            for k in (2, k_near):
                z_copy(m, b, k).start()

    def z_side(b):
        for m in range(2):
            z_copy(m, b, near_to).start()

    def z_down_side():
        for m in range(2):
            zd_copy(m, near_to).start()

    def z_down_cross():
        for m in range(2):
            for k in (2, k_near):
                zd_copy(m, k).start()

    load_tok = pltpu.make_async_copy(tok_in, raw, ld.at[0])
    loads = [pltpu.make_async_copy(src, stage.at[m], ld.at[1 + m]) for m, src in enumerate((gw, uw))]
    own_rows = pl.ds(row0(g, z), chunk)
    own_down = pltpu.make_async_copy(dw.at[z], dout.at[own_rows, :], ld.at[3])
    load_tok.start()
    for c in loads:
        c.start()
    own_down.start()

    barrier = pltpu.get_barrier_semaphore()
    for k in range(1, nz):
        pl.semaphore_signal(barrier, inc=1, device_id={"fs": to(k)}, device_id_type=MESH)
    for who in (mate, over):
        pl.semaphore_signal(barrier, inc=1, device_id={"tp": who}, device_id_type=MESH)
    pl.semaphore_signal(barrier, inc=1, device_id={"gr": 1 - g}, device_id_type=MESH)

    step = 64

    def norm():
        load_tok.wait()

        @pl.loop(0, rows // step)
        def _(i):
            at = pl.ds(pl.multiple_of(i * step, step), step)
            v = raw[at, :].astype(jnp.float32)
            scale = lax.rsqrt(jnp.mean(v * v, axis=-1, keepdims=True) + EPSILON)
            tok[z, at, :] = (v * scale).astype(jnp.bfloat16)

    norm()
    pl.semaphore_wait(barrier, nz - 1 + 3)

    guarded = []

    def guard(flag, c):
        @pl.when(flag)
        def _():
            c.start()
        guarded.append((flag, c))

    def hop(way, h, src):
        ref = tok.at[src, :, qcols(t)]
        nxt = lax.rem(z + way + nz, nz)
        return rdma(ref, ref, ts.at[(way + 1) // 2, h], tr.at[src], {"fs": nxt})

    right, left = z + 1 < nz, z >= 1
    for e in range(nz):
        wsend[e] = (
            jnp.where(routes[0:1, :] == e, rweight[0:1, :], 0.0)
            + jnp.where(routes[1:2, :] == e, rweight[1:2, :], 0.0)
        )
    wrecv[z] = wsend[z]
    for k in range(1, nz):
        rdma(wsend.at[to(k)], wrecv.at[z], gs.at[k], gr.at[k], {"fs": to(k)}).start()
    guard(right, hop(1, 0, z))
    guard(left, hop(-1, 0, z))
    for m in range(2):
        xd_own(m).start()

    def scaleall():
        gcol[...] = jnp.transpose(jnp.broadcast_to(gain[...], (128, chunk)))
        for c in loads:
            c.wait()

        @pl.loop(0, nz * (chunk // step))
        def _(i):
            e = i // (chunk // step)
            at = pl.ds(pl.multiple_of(lax.rem(i, chunk // step) * step, step), step)
            factor = jnp.concatenate([gcol[at, :]] * (width // 128), axis=1)
            for m in range(2):
                stage[m, e, at, :] = (stage[m, e, at, :].astype(jnp.float32) * factor).astype(jnp.bfloat16)

    scaleall()
    @pl.when(jnp.logical_not(inner))
    def _():
        pl.loop(0, nb)(z_side)
        pl.loop(0, nb)(z_cross)

    @pl.when(inner)
    def _():
        z_side(0)
        z_cross(0, (0,))

    for b in range(nb):
        for m in range(2):
            x_own(m, b).start()

    for m in range(2):
        outs[m][own_rows, :] = stage[m, z]
    before[...] = jnp.where(
        lax.broadcasted_iota(jnp.int32, (rows, rows), 0) < lax.broadcasted_iota(jnp.int32, (rows, rows), 1), 1.0, 0.0
    ).astype(jnp.bfloat16)

    def hops(h):
        for way in (1, -1):
            src = lax.rem(z - way * h + nz, nz)
            valid = z >= h if way == 1 else z + h < nz
            more = right if way == 1 else left
            ref = tok.at[src, :, qcols(t)]

            @pl.when(valid)
            def _(ref=ref, src=src):
                rdma(ref, ref, ts.at[0, 0], tr.at[src], {"fs": lax.rem(z + 1, nz)}).wait_recv()
            guard(jnp.logical_and(valid, more), hop(way, h, src))
            guard(valid, rdma(ref, ref, fs_s.at[1, src], fr.at[1, src], {"tp": over}))
            guard(valid, rdma(ref, ref, fs_s.at[0, src], fr.at[0, src], {"tp": mate}))

    def token_quarter(lane, src, q):
        ref = tok.at[src, :, qcols(q)]
        return rdma(ref, ref, fs_s.at[lane, src], fr.at[lane, src], {"tp": mate})

    def forward(s):
        src = frm(k_of(s))
        token_quarter(1, src, over).wait_recv()
        token_quarter(2, src, over).start()

    def tok_wait(src, s):
        token_quarter(0, src, mate).wait_recv()
        token_quarter(2, src, (1 - y) * 2 + 1 - core).wait_recv()
        rdma(wrecv.at[src], wrecv.at[src], gs.at[s], gr.at[s], {"fs": to(s)}).wait_recv()

    def prepare(s):
        src = frm(k_of(s))

        @pl.when(s >= 1)
        def _():
            tok_wait(src, k_of(s))
        weight = wrecv[src]
        chosen = weight != 0.0
        marks = jnp.broadcast_to(jnp.where(chosen, 1.0, 0.0), (16, rows)).astype(jnp.bfloat16)
        rank = jnp.dot(marks, before[...], preferred_element_type=jnp.float32)[0:1]
        key = jnp.where(chosen, rank, -1.0)
        match = key == lax.broadcasted_iota(jnp.int32, (cap, rows), 0).astype(jnp.float32)
        own_weight = jnp.sum(jnp.where(match, weight, 0.0), axis=1, keepdims=True)
        wcol[src] = jnp.broadcast_to(own_weight, (cap, 128))
        pick[...] = jnp.where(match, 1.0, 0.0).astype(jnp.bfloat16)
        column = jnp.transpose(jnp.broadcast_to(key, (128, rows)))
        lane = lax.broadcasted_iota(jnp.int32, (rows, 128), 1).astype(jnp.float32)
        for v in range(cap // 128):
            spread[src, :, v * 128:(v + 1) * 128] = jnp.where(column == lane + v * 128.0, 1.0, 0.0).astype(jnp.bfloat16)

        @pl.loop(0, nt)
        def _(q):
            packed[src, :, qcols(q)] = jnp.dot(
                pick[...], tok[src, :, qcols(q)], preferred_element_type=jnp.float32
            ).astype(jnp.bfloat16)

    def take_near(lo, hi):
        @pl.loop(lo, hi)
        def _(b):
            z_take(b, k_near)

    ends = jnp.logical_not(inner)
    hops(1)

    @pl.when(inner)
    def _():
        z_cross(0, (1,))
        take_near(0, nb // 2)

    @pl.when(ends)
    def _():
        z_take(0, k_near)
    hops(2)

    @pl.when(inner)
    def _():
        pl.loop(1, nb)(z_side)
        pl.loop(1, nb)(z_cross)
        z_down_side()
        z_down_cross()
        take_near(nb // 2, nb)

    @pl.when(ends)
    def _():
        z_take(0, k_far)
    for h in range(3, nz):
        hops(h)
    for s in (1, 3):
        forward(s)

    @pl.when(inner)
    def _():
        forward(2)
    pl.loop(0, 2)(prepare)

    @pl.loop(0, nb)
    def _(b):
        @pl.when(jnp.logical_or(inner, b >= 1))
        def _():
            z_take(b, k_far)

        @pl.when(jnp.logical_and(ends, lax.rem(b, 2) == 1))
        def _():
            z_take(b // 2 + 1, k_near)

        @pl.when(b == 0)
        def _():
            prepare(3)

            @pl.when(ends)
            def _():
                forward(2)

        @pl.when(b == 1)
        def _():
            prepare(2)

        @pl.when(b == nb // 2)
        def _():
            z_take(0, k_mid)

    def x_wait(b):
        @pl.loop(0, nz)
        def _(kk):
            for m in range(2):
                ref = piece(m, b, 1 - g, frm(kk))
                rdma(ref, ref, xs.at[m, b, kk], xr.at[m, b, kk], {"gr": 1 - g}).wait_recv()

    def hidden(b, src):
        a = packed[src]
        gate = jnp.dot(a, gout[:, cols(b)], preferred_element_type=jnp.float32)
        upper = jnp.dot(a, uout[:, cols(b)], preferred_element_type=jnp.float32)
        weight = jnp.concatenate([wcol[src]] * (blk // 128), axis=1)
        hid[src, :, cols(b)] = (gate / (1.0 + jnp.exp(-gate)) * upper * weight).astype(jnp.bfloat16)

    @pl.loop(nz, (nb + 1) * nz)
    def _(i):
        b, s = i // nz, lax.rem(i, nz)
        src = frm(k_of(s))

        @pl.when(jnp.logical_and(s == 0, b < nb))
        def _():
            z_take(b, k_mid)

        @pl.when(jnp.logical_and(jnp.logical_not(inner), jnp.logical_and(s == 1, b < nb - nb // 2)))
        def _():
            z_take(b + nb // 2, k_near)

        @pl.when(jnp.logical_and(jnp.logical_not(inner), i == (nb - 2) * nz))
        def _():
            z_down_side()

        @pl.when(i == nb * nz)
        def _():
            @pl.when(ends)
            def _():
                z_down_cross()
            zd_take(k_near)

        @pl.when(s == 0)
        def _():
            x_wait(b - 1)

        hidden(b - 1, src)

    own_down.wait()

    def chunk_of(i):
        k, other = k_of(i // 2), lax.rem(i, 2)
        group = g + other * (1 - 2 * g)
        c = group * nz + frm(k)
        owner = c // per_owner
        return k, other, c, owner, lax.rem(owner, 2), owner // 2, lax.rem(c, per_owner)

    def cut(ref, h):
        return ref if h is None else ref.at[:, pl.ds(h * half, half)]

    def slot_of(i, h):
        return i + 2 if h == 1 else i

    def give(i, j, h):
        k, other, c, owner, par, yo, cc = chunk_of(i)
        b, si = order_of(j), slot_of(i, h)
        src, dst = cut(part.at[c, b], h), cut(crx.at[yo * per_owner + cc, b], h)
        return rdma(src, dst, cs.at[si, j], cr.at[si, j], {"tp": mate})

    def up(i, j, h):
        k, other, c, owner, par, yo, cc = chunk_of(i)
        si = slot_of(i, h)
        src, dst = cut(part.at[c, order[j]], h), cut(yrx.at[cc, order[j]], h)
        return rdma(src, dst, ys.at[si, j], yr.at[si, j], {"tp": over})

    def near(cc, j, h):
        second = 1 if h == 1 else 0
        dst = rly.at[j, cc] if j < 2 else ret.at[0, cc]
        landed = hr.at[j, cc, second if j < 2 else 0]
        return rdma(cut(full.at[cc, order[j]], h), cut(dst, h), hs.at[j, cc, second], landed, {"fs": pair})

    def cross(cc, j, h):
        second = 1 if h == 1 else 0
        src, dst = cut(full.at[cc, order[j]], h), cut(ret.at[1, cc], h)
        return rdma(src, dst, rs.at[j, cc, second], rr.at[cc], {"fs": order[j]})

    def x_down_wait(k, ms):
        for m in ms:
            ref = dpiece(m, 1 - g, frm(k))
            rdma(ref, ref, xs.at[m, nb, k], xr.at[m, nb, k], {"gr": 1 - g}).wait_recv()

    n = chunks

    def stage_a(i):
        k, other, c, owner, par, yo, cc = chunk_of(i)

        @pl.when(other == 1)
        def _():
            x_down_wait(k, range(2))
        mine = pl.ds(pl.multiple_of(c * chunk, chunk), chunk)

        @pl.loop(0, nz)
        def _(j):
            b = order_of(j)
            part[c, b] = lax.dot_general(
                hid[b], dout[mine, :], (((1,), (1,)), ((), ())), preferred_element_type=jnp.float32
            ).astype(jnp.bfloat16)

            @pl.when(par != core)
            def _():
                give(i, j, None).start()

    def halves_a(i, h):
        k, other, c, owner, par, yo, cc = chunk_of(i)
        c2 = chunk_of(i + 1)[2]
        x_down_wait(k, (h,))
        mine = [pl.ds(pl.multiple_of(v * chunk + h * half, half), half) for v in (c, c2)]

        @pl.loop(0, nz)
        def _(j):
            b = order_of(j)
            both = lax.dot_general(
                hid[b], jnp.concatenate([dout[v, :] for v in mine], axis=0), (((1,), (1,)), ((), ())),
                preferred_element_type=jnp.float32,
            ).astype(jnp.bfloat16)
            cut(part.at[c, b], h)[...] = both[:, :half]
            cut(part.at[c2, b], h)[...] = both[:, half:]

            @pl.when(par != core)
            def _():
                give(i, j, h).start()
                give(i + 1, j, h).start()

    def add(target, h, ref):
        mine = cut(target, h)
        mine[...] = (mine[...].astype(jnp.float32) + ref[...].astype(jnp.float32)).astype(jnp.bfloat16)

    def stage_b(i, h=None):
        k, other, c, owner, par, yo, cc = chunk_of(i)
        si = slot_of(i, h)

        @pl.when(par == core)
        def _():
            for j in range(nz):
                b = order[j]
                ref = cut(crx.at[yo * per_owner + cc, b], h)
                rdma(ref, ref, cs.at[si, j], cr.at[si, j], {"tp": mate}).wait_recv()
                add(part.at[c, b], h, ref)

                @pl.when(yo != y)
                def _(j=j):
                    up(i, j, h).start()

    def stage_c(i, h=None):
        k, other, c, owner, par, yo, cc = chunk_of(i)
        si = slot_of(i, h)

        @pl.when(owner == t)
        def _():
            for j in range(nz):
                b = order[j]
                ref = cut(yrx.at[cc, b], h)
                rdma(ref, ref, ys.at[si, j], yr.at[si, j], {"tp": over}).wait_recv()
                total = cut(part.at[c, b], h)[...].astype(jnp.float32) + ref[...].astype(jnp.float32)
                cut(full.at[cc, b], h)[...] = jnp.dot(
                    spread[b], total.astype(jnp.bfloat16), preferred_element_type=jnp.float32
                ).astype(jnp.bfloat16)
                if j < 2:
                    @pl.when(jnp.logical_not(inner))
                    def _(j=j):
                        near(cc, j, h).start()
                elif j == 2 and h == 1:
                    near(cc, j, h).start()
                elif j == 2:
                    @pl.when(jnp.logical_or(inner, i < n - 4))
                    def _(j=j):
                        near(cc, j, h).start()

    def cross_phase(cc, h=None):
        for j in range(2):
            ref = cut(rly.at[j, cc], h)
            rdma(ref, ref, hs.at[j, cc, 0], hr.at[j, cc, 1 if h == 1 else 0], {"fs": pair}).wait_recv()
            add(full.at[cc, order[j]], h, ref)
            cross(cc, j, h).start()

    early = jnp.logical_and(inner, side == core)
    late = jnp.logical_and(inner, side != core)
    cc_far = lax.rem(frm(k_far), 2)

    @pl.loop(0, n - 2)
    def _(i):
        @pl.when(i == 3)
        def _():
            zd_take(k_far, (0,))

        @pl.when(i == 4)
        def _():
            zd_take(k_far, (1,))

        @pl.when(i == 5)
        def _():
            pl.loop(0, 2)(stage_c)

        @pl.when(jnp.logical_or(jnp.logical_and(ends, i == 4), jnp.logical_and(inner, i == 5)))
        def _():
            zd_take(k_mid, (0,))

        stage_a(i)
        stage_b(i)

    pl.loop(2, 4)(stage_c)

    def last(h):
        halves_a(n - 2, h)

        @pl.loop(n - 2, n)
        def _(i):
            stage_b(i, h)

    @pl.when(ends)
    def _():
        zd_take(k_mid, (1,))
    last(0)

    @pl.when(inner)
    def _():
        zd_take(k_mid, (1,))

    @pl.when(early)
    def _():
        pl.loop(0, per_owner)(cross_phase)
    pl.loop(n - 4, n - 2)(stage_c)

    last(1)

    @pl.when(late)
    def _():
        cross_phase(cc_far)
    for h in range(2):
        @pl.loop(n - 2, n)
        def _(i, h=h):
            stage_c(i, h)

        @pl.when(late)
        def _(h=h):
            cross_phase(1 - cc_far, h)

    @pl.when(jnp.logical_and(ends, side != core))
    def _():
        near(cc_far, 2, None).start()
        near(1 - cc_far, 2, 0).start()

    def final():
        for cc in range(per_owner):
            direct, crossed = ret.at[0, cc], ret.at[1, cc]
            rdma(direct, direct, hs.at[2, cc, 0], hr.at[2, cc, 0], {"fs": pair}).wait_recv()
            rdma(crossed, crossed, rs.at[0, cc, 0], rr.at[cc], {"fs": pair}).wait_recv()
            mixed[:, cc * chunk:(cc + 1) * chunk] = (
                full[cc, z].astype(jnp.float32)
                + ret[0, cc].astype(jnp.float32)
                + ret[1, cc].astype(jnp.float32)
            ).astype(jnp.bfloat16)

    final()

    def send_waits():
        @pl.loop(1, nz)
        def _(k):
            rdma(wsend.at[to(k)], wrecv.at[z], gs.at[k], gr.at[k], {"fs": to(k)}).wait_send()
            for m in range(2):
                zd_copy(m, k).wait_send()
                relay(dpiece(m, g, frm(k)), m, nb, k).wait_send()
            token_quarter(2, frm(k), over).wait_send()

            @pl.loop(0, nb)
            def _(b):
                for m in range(2):
                    z_copy(m, b, k).wait_send()
                    relay(piece(m, b, g, frm(k)), m, b, k).wait_send()

        for m in range(2):
            xd_own(m).wait_send()

            @pl.loop(0, nb)
            def _(b):
                x_own(m, b).wait_send()

        for flag, c in guarded:
            @pl.when(flag)
            def _(c=c):
                c.wait_send()

        def sent(i, h):
            k, other, c, owner, par, yo, cc = chunk_of(i)

            @pl.when(par != core)
            def _():
                for j in range(nz):
                    give(i, j, h).wait_send()

            @pl.when(jnp.logical_and(par == core, yo != y))
            def _():
                for j in range(nz):
                    up(i, j, h).wait_send()

        def returned(cc, h):
            near(cc, 2, h).wait_send()
            for j in range(2):
                @pl.when(inner)
                def _(j=j):
                    cross(cc, j, h).wait_send()

                @pl.when(jnp.logical_not(inner))
                def _(j=j):
                    near(cc, j, h).wait_send()

        @pl.loop(0, n - 2)
        def _(i):
            sent(i, None)
        for h in range(2):
            @pl.loop(n - 2, n)
            def _(i, h=h):
                sent(i, h)
        returned(cc_far, None)

        @pl.when(side == core)
        def _():
            returned(1 - cc_far, None)

        @pl.when(side != core)
        def _():
            for h in range(2):
                returned(1 - cc_far, h)

    send_waits()


def store(gate, upper, down, mixed, gate_out, up_out, down_out, mixed_out, sem):
    copies = [
        pltpu.make_async_copy(gate, gate_out.at[0], sem.at[0]),
        pltpu.make_async_copy(upper, up_out.at[0], sem.at[1]),
        pltpu.make_async_copy(down, down_out.at[0], sem.at[2]),
        pltpu.make_async_copy(mixed, mixed_out, sem.at[3]),
    ]
    for c in copies:
        c.start()
    for c in copies:
        c.wait()


def fused(ng, nz, nt, tokens, routes, route_weight, gain, w_gate, w_up, w_down):
    rows, d = tokens.shape
    quarter = d // nt
    experts, chunk, width = w_gate.shape
    chunks = ng * nz
    per_owner = chunks // nt
    cap = 3 * rows // experts
    bf, f32 = jnp.bfloat16, jnp.float32
    dma = pltpu.SemaphoreType.DMA
    full = pltpu.VMEM((d, width), bf)
    vmem = pl.BlockSpec(memory_space=pltpu.VMEM)
    anywhere = pl.BlockSpec(memory_space=pl.ANY)
    results = pl.pallas_call(
        functools.partial(kernel, ng, nz, nt),
        out_shape=(full, full, full, pltpu.VMEM((rows, quarter), bf)),
        in_specs=[anywhere, vmem, vmem, vmem, anywhere, anywhere, anywhere],
        out_specs=(vmem,) * 4,
        scratch_shapes=[
            pltpu.VMEM((nz, rows, d), bf),
            pltpu.VMEM((nz, cap, d), bf),
            pltpu.VMEM((nz, cap, width), bf),
            pltpu.VMEM((chunks, nz, cap, chunk), bf),
            pltpu.VMEM((chunks // 2, nz, cap, chunk), bf),
            pltpu.VMEM((per_owner, nz, cap, chunk), bf),
            pltpu.VMEM((per_owner, nz, rows, chunk), bf),
            pltpu.VMEM((2, nz, chunk, width), bf),
            pltpu.VMEM((rows, d), bf),
            pltpu.VMEM((2, per_owner, rows, chunk), bf),
            pltpu.VMEM((2, per_owner, rows, chunk), bf),
            pltpu.VMEM((nz, 1, rows), f32),
            pltpu.VMEM((nz, 1, rows), f32),
            pltpu.VMEM((nz, cap, 128), f32),
            pltpu.VMEM((chunk, 128), f32),
            pltpu.VMEM((rows, rows), bf),
            pltpu.VMEM((cap, rows), bf),
            pltpu.VMEM((nz, rows, cap), bf),
            dma((4,)),
            dma((2, nz)), dma((nz,)),
            dma((3, nz)), dma((3, nz)),
            dma((nz,)), dma((nz,)),
            dma((2, BLOCKS + 1, nz)), dma((2, BLOCKS + 1, nz)),
            dma((2, BLOCKS + 1, nz)), dma((2, BLOCKS + 1, nz)),
            dma((chunks + 2, nz)), dma((chunks + 2, nz)),
            dma((chunks + 2, nz)), dma((chunks + 2, nz)),
            dma((3, per_owner, 2)), dma((3, per_owner, 2)),
            dma((2, per_owner, 2)), dma((per_owner,)),
        ],
        compiler_params=pltpu.CompilerParams(
            collective_id=0, has_side_effects=True, vmem_limit_bytes=VMEM_LIMIT
        ),
    )(tokens, routes.T, route_weight.T, gain.reshape(1, chunk), w_gate, w_up, w_down)
    whole = jax.ShapeDtypeStruct((1, d, width), bf)
    return pl.pallas_call(
        store,
        out_shape=(whole, whole, whole, jax.ShapeDtypeStruct((rows, quarter), bf)),
        in_specs=[vmem] * 4,
        out_specs=(anywhere,) * 4,
        scratch_shapes=[dma((4,))],
        compiler_params=pltpu.CompilerParams(vmem_limit_bytes=4 * 1024 * 1024),
    )(*results)

EXP_DEV = 1


def body(tokens, routes, route_weight, gain, w_gate, w_up, w_down):
    scaling = gain[None, :, None]
    gate_local = (w_gate * scaling).astype(jnp.bfloat16)
    up_local = (w_up * scaling).astype(jnp.bfloat16)
    gate_mine, up_mine, down_mine = (
        lax.all_to_all(gate_local, "fs", split_axis=0, concat_axis=1, tiled=True),
        lax.all_to_all(up_local, "fs", split_axis=0, concat_axis=1, tiled=True),
        lax.all_to_all(w_down, "fs", split_axis=0, concat_axis=1, tiled=True),
    )
    gate_out, up_out, down_out = (
        lax.all_gather(gate_mine, "gr", axis=1, tiled=True),
        lax.all_gather(up_mine, "gr", axis=1, tiled=True),
        lax.all_gather(down_mine, "gr", axis=1, tiled=True),
    )
    fs_count = lax.axis_size("fs")
    experts = EXP_DEV * fs_count
    tok_rows = tokens.shape[0]
    capacity = 3 * tok_rows // experts
    float_rows = tokens.astype(jnp.float32)
    normed = (
        float_rows * lax.rsqrt(jnp.mean(float_rows * float_rows, axis=-1, keepdims=True) + EPSILON)
    ).astype(jnp.bfloat16)
    flat_ids = routes.reshape(-1)
    onehot = (flat_ids[:, None] == jnp.arange(experts, dtype=jnp.int32)[None, :]).astype(jnp.int32)
    slot_rank = jnp.sum((jnp.cumsum(onehot, axis=0) - onehot) * onehot, axis=-1)
    destination = (flat_ids * capacity + slot_rank).reshape(tok_rows, 2)
    slot_ids = jnp.arange(experts * capacity, dtype=jnp.int32)
    hits = slot_ids[:, None, None] == destination[None, :, :]
    dispatch = jnp.any(hits, axis=-1).astype(jnp.bfloat16)
    outgoing = jnp.dot(dispatch, normed, preferred_element_type=jnp.float32).astype(jnp.bfloat16)
    outgoing = outgoing.reshape(fs_count, EXP_DEV, capacity, tokens.shape[1])
    arrived = lax.all_to_all(outgoing, "fs", split_axis=0, concat_axis=0, tiled=True)
    gate = jnp.einsum("sjnd,jdf->sjnf", arrived, gate_out, preferred_element_type=jnp.float32)
    upper = jnp.einsum("sjnd,jdf->sjnf", arrived, up_out, preferred_element_type=jnp.float32)
    hidden = (jax.nn.silu(gate) * upper).astype(jnp.bfloat16)
    partial_value = jnp.einsum(
        "sjnf,jdf->sjnd", hidden, down_out, preferred_element_type=jnp.float32
    )
    rounded = lax.optimization_barrier(partial_value.astype(jnp.bfloat16))
    summed = lax.psum_scatter(
        rounded.astype(jnp.float32).astype(jnp.bfloat16), "tp", scatter_dimension=3, tiled=True
    )
    back_home = lax.all_to_all(summed, "fs", split_axis=0, concat_axis=0, tiled=True)
    features = back_home.shape[-1]
    flat_back = back_home.reshape(experts * capacity, features).astype(jnp.float32)
    first = jnp.where(slot_ids[None, :] == destination[:, 0:1], route_weight[:, 0:1], 0.0)
    second = jnp.where(slot_ids[None, :] == destination[:, 1:2], route_weight[:, 1:2], 0.0)
    combine_map = first + second
    mixed = jnp.dot(
        combine_map, flat_back, precision=lax.Precision.HIGHEST, preferred_element_type=jnp.float32
    ).astype(jnp.bfloat16)
    return (gate_out, up_out, down_out, mixed)


def solution(mesh):
    in_specs = (
        P(("gr", "fs"), None),
        P(("gr", "fs"), None),
        P(("gr", "fs"), None),
        P(("gr", "fs")),
        P(None, ("gr", "fs"), "tp"),
        P(None, ("gr", "fs"), "tp"),
        P(None, ("gr", "fs"), "tp"),
    )
    out_specs = (
        P("fs", None, "tp"),
        P("fs", None, "tp"),
        P("fs", None, "tp"),
        P(("gr", "fs"), "tp"),
    )
    ng, nz, nt = mesh.shape["gr"], mesh.shape["fs"], mesh.shape["tp"]
    small = ng == 2 and nt == 4 and nz == 4
    work = functools.partial(fused, ng, nz, nt) if small else body
    return jax.shard_map(work, mesh=mesh, in_specs=in_specs, out_specs=out_specs, check_vma=False)
```

```python
import functools
import jax
import jax.numpy as jnp
from jax import lax
from jax.experimental import pallas as pl
from jax.experimental.pallas import tpu as pltpu
from jax.sharding import PartitionSpec as P

MESH = pl.DeviceIdType.MESH
VMEM_LIMIT = 50 * 1024 * 1024
EPSILON = 1e-05
BLOCKS = 4
LAG = 4


def kernel(ng, nz, nt, tok_in, routes, rweight, gain, gw, uw, dw, gout, uout, dout, mixed,
           tok, packed, hid, part, crx, yrx, full, stage, raw, ret, rly, wsend, wrecv, wcol, gcol, before, pick, spread,
           ld, ts, tr, fs_s, fr, gs, gr, zs, zr, xs, xr, cs, cr, ys, yr, hs, hr, rs, rr):
    g, z, t = lax.axis_index("gr"), lax.axis_index("fs"), lax.axis_index("tp")
    core, y = lax.rem(t, 2), lax.div(t, 2)
    rows, d = tok_in.shape
    quarter = d // nt
    chunk, width = gw.shape[1], gw.shape[2]
    half = chunk // 2
    cap = packed.shape[1]
    chunks = ng * nz
    per_owner = chunks // nt
    nb = BLOCKS
    blk = width // nb
    outs = (gout, uout)
    mate, over = y * 2 + 1 - core, (1 - y) * 2 + core
    inner = jnp.logical_and(z > 0, z < nz - 1)
    side = lax.div(z, 2)
    pair = z + 1 - 2 * lax.rem(z, 2)
    far = (3 * (1 - side), 2 - side)
    order = (far[0], far[1], pair, z)
    odd = lax.rem(z, 2)
    k_near = 3 - 2 * odd
    near_to = 4 - k_near
    k_mid = jnp.where(inner, near_to, 2)
    k_far = jnp.where(inner, 2, near_to)

    def to(k):
        return lax.rem(z + k, nz)

    def frm(k):
        return lax.rem(z + nz - k, nz)

    def rdma(src, dst, ss, rsem, dev):
        return pltpu.make_async_remote_copy(
            src_ref=src, dst_ref=dst, send_sem=ss, recv_sem=rsem, device_id=dev, device_id_type=MESH
        )

    def row0(group, zsrc):
        return pl.multiple_of((group * nz + zsrc) * chunk, chunk)

    def cols(b):
        return pl.ds(pl.multiple_of(b * blk, blk), blk)

    def qcols(q):
        return pl.ds(pl.multiple_of(q * quarter, quarter), quarter)

    def piece(m, b, group, zsrc):
        return outs[m].at[pl.ds(row0(group, zsrc), chunk), cols(b)]

    def dpiece(m, group, zsrc):
        return dout.at[pl.ds(pl.multiple_of(row0(group, zsrc) + m * half, half), half), :]

    def z_copy(m, b, k):
        return rdma(stage.at[m, to(k), :, cols(b)], piece(m, b, g, z), zs.at[m, b, k], zr.at[m, b, k], {"fs": to(k)})

    def zd_copy(m, k):
        return rdma(dw.at[to(k), pl.ds(m * half, half), :], dpiece(m, g, z), zs.at[m, nb, k], zr.at[m, nb, k], {"fs": to(k)})

    def x_own(m, b):
        return rdma(stage.at[m, z, :, cols(b)], piece(m, b, g, z), xs.at[m, b, 0], xr.at[m, b, 0], {"gr": 1 - g})

    def xd_own(m):
        return rdma(dw.at[z, pl.ds(m * half, half), :], dpiece(m, g, z), xs.at[m, nb, 0], xr.at[m, nb, 0], {"gr": 1 - g})

    def relay(ref, m, b, k):
        return rdma(ref, ref, xs.at[m, b, k], xr.at[m, b, k], {"gr": 1 - g})

    def z_arrive(ref, m, b, k):
        rdma(ref, ref, zs.at[m, b, k], zr.at[m, b, k], {"fs": to(k)}).wait_recv()

    def z_take(b, k):
        for m in range(2):
            ref = piece(m, b, g, frm(k))
            z_arrive(ref, m, b, k)
            relay(ref, m, b, k).start()

    def zd_take(k, ms=(0, 1)):
        for m in ms:
            ref = dpiece(m, g, frm(k))
            z_arrive(ref, m, nb, k)
            relay(ref, m, nb, k).start()

    def order_of(j):
        return jnp.where(j == 0, far[0], jnp.where(j == 1, far[1], jnp.where(j == 2, pair, z)))

    def k_of(s):
        return jnp.where(s == 0, 0, jnp.where(s == 1, k_near, jnp.where(s == 2, k_far, k_mid)))

    def z_cross(b, ms=(0, 1)):
        for m in ms:
            for k in (2, k_near):
                z_copy(m, b, k).start()

    def z_side(b):
        for m in range(2):
            z_copy(m, b, near_to).start()

    def z_down_side():
        for m in range(2):
            zd_copy(m, near_to).start()

    def z_down_cross():
        for m in range(2):
            for k in (2, k_near):
                zd_copy(m, k).start()

    load_tok = pltpu.make_async_copy(tok_in, raw, ld.at[0])
    loads = [pltpu.make_async_copy(src, stage.at[m], ld.at[1 + m]) for m, src in enumerate((gw, uw))]
    own_rows = pl.ds(row0(g, z), chunk)
    own_down = pltpu.make_async_copy(dw.at[z], dout.at[own_rows, :], ld.at[3])
    load_tok.start()
    for c in loads:
        c.start()
    own_down.start()

    barrier = pltpu.get_barrier_semaphore()
    for k in range(1, nz):
        pl.semaphore_signal(barrier, inc=1, device_id={"fs": to(k)}, device_id_type=MESH)
    for who in (mate, over):
        pl.semaphore_signal(barrier, inc=1, device_id={"tp": who}, device_id_type=MESH)
    pl.semaphore_signal(barrier, inc=1, device_id={"gr": 1 - g}, device_id_type=MESH)

    step = 64

    def norm():
        load_tok.wait()

        @pl.loop(0, rows // step)
        def _(i):
            at = pl.ds(pl.multiple_of(i * step, step), step)
            v = raw[at, :].astype(jnp.float32)
            scale = lax.rsqrt(jnp.mean(v * v, axis=-1, keepdims=True) + EPSILON)
            tok[z, at, :] = (v * scale).astype(jnp.bfloat16)

    norm()
    pl.semaphore_wait(barrier, nz - 1 + 3)

    guarded = []

    def guard(flag, c):
        @pl.when(flag)
        def _():
            c.start()
        guarded.append((flag, c))

    def hop(way, h, src):
        ref = tok.at[src, :, qcols(t)]
        nxt = lax.rem(z + way + nz, nz)
        return rdma(ref, ref, ts.at[(way + 1) // 2, h], tr.at[src], {"fs": nxt})

    right, left = z + 1 < nz, z >= 1
    for e in range(nz):
        wsend[e] = (
            jnp.where(routes[0:1, :] == e, rweight[0:1, :], 0.0)
            + jnp.where(routes[1:2, :] == e, rweight[1:2, :], 0.0)
        )
    wrecv[z] = wsend[z]
    for k in range(1, nz):
        rdma(wsend.at[to(k)], wrecv.at[z], gs.at[k], gr.at[k], {"fs": to(k)}).start()
    guard(right, hop(1, 0, z))
    guard(left, hop(-1, 0, z))
    for m in range(2):
        xd_own(m).start()

    def scaleall():
        gcol[...] = jnp.transpose(jnp.broadcast_to(gain[...], (128, chunk)))
        for c in loads:
            c.wait()

        @pl.loop(0, nz * (chunk // step))
        def _(i):
            e = i // (chunk // step)
            at = pl.ds(pl.multiple_of(lax.rem(i, chunk // step) * step, step), step)
            factor = jnp.concatenate([gcol[at, :]] * (width // 128), axis=1)
            for m in range(2):
                stage[m, e, at, :] = (stage[m, e, at, :].astype(jnp.float32) * factor).astype(jnp.bfloat16)

    scaleall()
    @pl.when(jnp.logical_not(inner))
    def _():
        pl.loop(0, nb)(z_side)
        pl.loop(0, nb)(z_cross)

    @pl.when(inner)
    def _():
        z_side(0)
        z_cross(0, (0,))

    for b in range(nb):
        for m in range(2):
            x_own(m, b).start()

    for m in range(2):
        outs[m][own_rows, :] = stage[m, z]
    before[...] = jnp.where(
        lax.broadcasted_iota(jnp.int32, (rows, rows), 0) < lax.broadcasted_iota(jnp.int32, (rows, rows), 1), 1.0, 0.0
    ).astype(jnp.bfloat16)

    def hops(h):
        for way in (1, -1):
            src = lax.rem(z - way * h + nz, nz)
            valid = z >= h if way == 1 else z + h < nz
            more = right if way == 1 else left
            ref = tok.at[src, :, qcols(t)]

            @pl.when(valid)
            def _(ref=ref, src=src):
                rdma(ref, ref, ts.at[0, 0], tr.at[src], {"fs": lax.rem(z + 1, nz)}).wait_recv()
            guard(jnp.logical_and(valid, more), hop(way, h, src))
            guard(valid, rdma(ref, ref, fs_s.at[1, src], fr.at[1, src], {"tp": over}))
            guard(valid, rdma(ref, ref, fs_s.at[0, src], fr.at[0, src], {"tp": mate}))

    def token_quarter(lane, src, q):
        ref = tok.at[src, :, qcols(q)]
        return rdma(ref, ref, fs_s.at[lane, src], fr.at[lane, src], {"tp": mate})

    def forward(s):
        src = frm(k_of(s))
        token_quarter(1, src, over).wait_recv()
        token_quarter(2, src, over).start()

    def tok_wait(src, s):
        token_quarter(0, src, mate).wait_recv()
        token_quarter(2, src, (1 - y) * 2 + 1 - core).wait_recv()
        rdma(wrecv.at[src], wrecv.at[src], gs.at[s], gr.at[s], {"fs": to(s)}).wait_recv()

    def prepare(s):
        src = frm(k_of(s))

        @pl.when(s >= 1)
        def _():
            tok_wait(src, k_of(s))
        weight = wrecv[src]
        chosen = weight != 0.0
        marks = jnp.broadcast_to(jnp.where(chosen, 1.0, 0.0), (16, rows)).astype(jnp.bfloat16)
        rank = jnp.dot(marks, before[...], preferred_element_type=jnp.float32)[0:1]
        key = jnp.where(chosen, rank, -1.0)
        match = key == lax.broadcasted_iota(jnp.int32, (cap, rows), 0).astype(jnp.float32)
        own_weight = jnp.sum(jnp.where(match, weight, 0.0), axis=1, keepdims=True)
        wcol[src] = jnp.broadcast_to(own_weight, (cap, 128))
        pick[...] = jnp.where(match, 1.0, 0.0).astype(jnp.bfloat16)
        column = jnp.transpose(jnp.broadcast_to(key, (128, rows)))
        lane = lax.broadcasted_iota(jnp.int32, (rows, 128), 1).astype(jnp.float32)
        for v in range(cap // 128):
            spread[src, :, v * 128:(v + 1) * 128] = jnp.where(column == lane + v * 128.0, 1.0, 0.0).astype(jnp.bfloat16)

        @pl.loop(0, nt)
        def _(q):
            packed[src, :, qcols(q)] = jnp.dot(
                pick[...], tok[src, :, qcols(q)], preferred_element_type=jnp.float32
            ).astype(jnp.bfloat16)

    def take_near(lo, hi):
        @pl.loop(lo, hi)
        def _(b):
            z_take(b, k_near)

    ends = jnp.logical_not(inner)
    hops(1)

    @pl.when(inner)
    def _():
        z_cross(0, (1,))
        take_near(0, nb // 2)

    @pl.when(ends)
    def _():
        z_take(0, k_near)
    hops(2)

    @pl.when(inner)
    def _():
        pl.loop(1, nb)(z_side)
        pl.loop(1, nb)(z_cross)
        z_down_side()
        z_down_cross()
        take_near(nb // 2, nb)

    @pl.when(ends)
    def _():
        z_take(0, k_far)
    for h in range(3, nz):
        hops(h)
    for s in (1, 3):
        forward(s)

    @pl.when(inner)
    def _():
        forward(2)
    pl.loop(0, 2)(prepare)

    @pl.loop(0, nb)
    def _(b):
        @pl.when(jnp.logical_or(inner, b >= 1))
        def _():
            z_take(b, k_far)

        @pl.when(jnp.logical_and(ends, lax.rem(b, 2) == 1))
        def _():
            z_take(b // 2 + 1, k_near)

        @pl.when(b == 0)
        def _():
            prepare(3)

            @pl.when(ends)
            def _():
                forward(2)

        @pl.when(b == 1)
        def _():
            prepare(2)

        @pl.when(b == nb // 2)
        def _():
            z_take(0, k_mid)

    def x_wait(b):
        @pl.loop(0, nz)
        def _(kk):
            for m in range(2):
                ref = piece(m, b, 1 - g, frm(kk))
                rdma(ref, ref, xs.at[m, b, kk], xr.at[m, b, kk], {"gr": 1 - g}).wait_recv()

    def hidden(b, src):
        a = packed[src]
        gate = jnp.dot(a, gout[:, cols(b)], preferred_element_type=jnp.float32)
        upper = jnp.dot(a, uout[:, cols(b)], preferred_element_type=jnp.float32)
        weight = jnp.concatenate([wcol[src]] * (blk // 128), axis=1)
        hid[src, :, cols(b)] = (gate / (1.0 + jnp.exp(-gate)) * upper * weight).astype(jnp.bfloat16)

    @pl.loop(nz, (nb + 1) * nz)
    def _(i):
        b, s = i // nz, lax.rem(i, nz)
        src = frm(k_of(s))

        @pl.when(jnp.logical_and(s == 0, b < nb))
        def _():
            z_take(b, k_mid)

        @pl.when(jnp.logical_and(jnp.logical_not(inner), jnp.logical_and(s == 1, b < nb - nb // 2)))
        def _():
            z_take(b + nb // 2, k_near)

        @pl.when(jnp.logical_and(jnp.logical_not(inner), i == (nb - 2) * nz))
        def _():
            z_down_side()

        @pl.when(jnp.logical_and(ends, i == nb * nz - 3))
        def _():
            z_down_cross()

        @pl.when(i == nb * nz)
        def _():
            zd_take(k_near)

        @pl.when(s == 0)
        def _():
            x_wait(b - 1)

        hidden(b - 1, src)

    own_down.wait()

    def chunk_of(i):
        k, other = k_of(i // 2), lax.rem(i, 2)
        group = g + other * (1 - 2 * g)
        c = group * nz + frm(k)
        owner = c // per_owner
        return k, other, c, owner, lax.rem(owner, 2), owner // 2, lax.rem(c, per_owner)

    def cut(ref, h):
        return ref if h is None else ref.at[:, pl.ds(h * half, half)]

    def slot_of(i, h):
        return i + 2 if h == 1 else i

    def give(i, j, h):
        k, other, c, owner, par, yo, cc = chunk_of(i)
        b, si = order_of(j), slot_of(i, h)
        src, dst = cut(part.at[c, b], h), cut(crx.at[yo * per_owner + cc, b], h)
        return rdma(src, dst, cs.at[si, j], cr.at[si, j], {"tp": mate})

    def up(i, j, h):
        k, other, c, owner, par, yo, cc = chunk_of(i)
        si = slot_of(i, h)
        src, dst = cut(part.at[c, order[j]], h), cut(yrx.at[cc, order[j]], h)
        return rdma(src, dst, ys.at[si, j], yr.at[si, j], {"tp": over})

    def near(cc, j, h):
        second = 1 if h == 1 else 0
        dst = rly.at[j, cc] if j < 2 else ret.at[0, cc]
        landed = hr.at[j, cc, second if j < 2 else 0]
        return rdma(cut(full.at[cc, order[j]], h), cut(dst, h), hs.at[j, cc, second], landed, {"fs": pair})

    def cross(cc, j, h):
        second = 1 if h == 1 else 0
        src, dst = cut(full.at[cc, order[j]], h), cut(ret.at[1, cc], h)
        return rdma(src, dst, rs.at[j, cc, second], rr.at[cc], {"fs": order[j]})

    def x_down_wait(k, ms):
        for m in ms:
            ref = dpiece(m, 1 - g, frm(k))
            rdma(ref, ref, xs.at[m, nb, k], xr.at[m, nb, k], {"gr": 1 - g}).wait_recv()

    n = chunks

    def stage_a(i):
        k, other, c, owner, par, yo, cc = chunk_of(i)

        @pl.when(other == 1)
        def _():
            x_down_wait(k, range(2))
        mine = pl.ds(pl.multiple_of(c * chunk, chunk), chunk)

        @pl.loop(0, nz)
        def _(j):
            b = order_of(j)
            part[c, b] = lax.dot_general(
                hid[b], dout[mine, :], (((1,), (1,)), ((), ())), preferred_element_type=jnp.float32
            ).astype(jnp.bfloat16)

            @pl.when(par != core)
            def _():
                give(i, j, None).start()

    def halves_a(i, h):
        k, other, c, owner, par, yo, cc = chunk_of(i)
        c2 = chunk_of(i + 1)[2]
        x_down_wait(k, (h,))
        mine = [pl.ds(pl.multiple_of(v * chunk + h * half, half), half) for v in (c, c2)]

        @pl.loop(0, nz)
        def _(j):
            b = order_of(j)
            both = lax.dot_general(
                hid[b], jnp.concatenate([dout[v, :] for v in mine], axis=0), (((1,), (1,)), ((), ())),
                preferred_element_type=jnp.float32,
            ).astype(jnp.bfloat16)
            cut(part.at[c, b], h)[...] = both[:, :half]
            cut(part.at[c2, b], h)[...] = both[:, half:]

            @pl.when(par != core)
            def _():
                give(i, j, h).start()
                give(i + 1, j, h).start()

    def add(target, h, ref):
        mine = cut(target, h)
        mine[...] = (mine[...].astype(jnp.float32) + ref[...].astype(jnp.float32)).astype(jnp.bfloat16)

    def stage_b(i, h=None):
        k, other, c, owner, par, yo, cc = chunk_of(i)
        si = slot_of(i, h)

        @pl.when(par == core)
        def _():
            for j in range(nz):
                b = order[j]
                ref = cut(crx.at[yo * per_owner + cc, b], h)
                rdma(ref, ref, cs.at[si, j], cr.at[si, j], {"tp": mate}).wait_recv()
                add(part.at[c, b], h, ref)

                @pl.when(yo != y)
                def _(j=j):
                    up(i, j, h).start()

    def stage_c(i, h=None):
        k, other, c, owner, par, yo, cc = chunk_of(i)
        si = slot_of(i, h)

        @pl.when(owner == t)
        def _():
            for j in range(nz):
                b = order[j]
                ref = cut(yrx.at[cc, b], h)
                rdma(ref, ref, ys.at[si, j], yr.at[si, j], {"tp": over}).wait_recv()
                total = cut(part.at[c, b], h)[...].astype(jnp.float32) + ref[...].astype(jnp.float32)
                cut(full.at[cc, b], h)[...] = jnp.dot(
                    spread[b], total.astype(jnp.bfloat16), preferred_element_type=jnp.float32
                ).astype(jnp.bfloat16)
                if j < 2:
                    @pl.when(jnp.logical_not(inner))
                    def _(j=j):
                        near(cc, j, h).start()
                elif j == 2 and h == 1:
                    near(cc, j, h).start()
                elif j == 2:
                    @pl.when(jnp.logical_or(inner, i < n - 4))
                    def _(j=j):
                        near(cc, j, h).start()

    def cross_phase(cc, h=None):
        for j in range(2):
            ref = cut(rly.at[j, cc], h)
            rdma(ref, ref, hs.at[j, cc, 0], hr.at[j, cc, 1 if h == 1 else 0], {"fs": pair}).wait_recv()
            add(full.at[cc, order[j]], h, ref)
            cross(cc, j, h).start()

    early = jnp.logical_and(inner, side == core)
    late = jnp.logical_and(inner, side != core)
    cc_far = lax.rem(frm(k_far), 2)

    @pl.loop(0, n - 2)
    def _(i):
        @pl.when(i == 3)
        def _():
            zd_take(k_far, (0,))

        @pl.when(i == 4)
        def _():
            zd_take(k_far, (1,))

        @pl.when(i == 5)
        def _():
            pl.loop(0, 2)(stage_c)

        @pl.when(jnp.logical_and(ends, i == 4))
        def _():
            zd_take(k_mid, (0,))

        stage_a(i)
        stage_b(i)

    @pl.when(inner)
    def _():
        zd_take(k_mid, (0,))
    pl.loop(2, 4)(stage_c)

    def last(h):
        halves_a(n - 2, h)

        @pl.loop(n - 2, n)
        def _(i):
            stage_b(i, h)

    @pl.when(ends)
    def _():
        zd_take(k_mid, (1,))
    last(0)

    @pl.when(inner)
    def _():
        zd_take(k_mid, (1,))

    @pl.when(early)
    def _():
        pl.loop(0, per_owner)(cross_phase)
    pl.loop(n - 4, n - 2)(stage_c)

    last(1)

    @pl.when(late)
    def _():
        cross_phase(cc_far)
    for h in range(2):
        @pl.loop(n - 2, n)
        def _(i, h=h):
            stage_c(i, h)

        @pl.when(late)
        def _(h=h):
            cross_phase(1 - cc_far, h)

    @pl.when(jnp.logical_and(ends, side != core))
    def _():
        near(cc_far, 2, None).start()
        near(1 - cc_far, 2, 0).start()

    def final():
        for cc in range(per_owner):
            direct, crossed = ret.at[0, cc], ret.at[1, cc]
            rdma(direct, direct, hs.at[2, cc, 0], hr.at[2, cc, 0], {"fs": pair}).wait_recv()
            rdma(crossed, crossed, rs.at[0, cc, 0], rr.at[cc], {"fs": pair}).wait_recv()
            mixed[:, cc * chunk:(cc + 1) * chunk] = (
                full[cc, z].astype(jnp.float32)
                + ret[0, cc].astype(jnp.float32)
                + ret[1, cc].astype(jnp.float32)
            ).astype(jnp.bfloat16)

    final()

    def send_waits():
        @pl.loop(1, nz)
        def _(k):
            rdma(wsend.at[to(k)], wrecv.at[z], gs.at[k], gr.at[k], {"fs": to(k)}).wait_send()
            for m in range(2):
                zd_copy(m, k).wait_send()
                relay(dpiece(m, g, frm(k)), m, nb, k).wait_send()
            token_quarter(2, frm(k), over).wait_send()

            @pl.loop(0, nb)
            def _(b):
                for m in range(2):
                    z_copy(m, b, k).wait_send()
                    relay(piece(m, b, g, frm(k)), m, b, k).wait_send()

        for m in range(2):
            xd_own(m).wait_send()

            @pl.loop(0, nb)
            def _(b):
                x_own(m, b).wait_send()

        for flag, c in guarded:
            @pl.when(flag)
            def _(c=c):
                c.wait_send()

        def sent(i, h):
            k, other, c, owner, par, yo, cc = chunk_of(i)

            @pl.when(par != core)
            def _():
                for j in range(nz):
                    give(i, j, h).wait_send()

            @pl.when(jnp.logical_and(par == core, yo != y))
            def _():
                for j in range(nz):
                    up(i, j, h).wait_send()

        def returned(cc, h):
            near(cc, 2, h).wait_send()
            for j in range(2):
                @pl.when(inner)
                def _(j=j):
                    cross(cc, j, h).wait_send()

                @pl.when(jnp.logical_not(inner))
                def _(j=j):
                    near(cc, j, h).wait_send()

        @pl.loop(0, n - 2)
        def _(i):
            sent(i, None)
        for h in range(2):
            @pl.loop(n - 2, n)
            def _(i, h=h):
                sent(i, h)
        returned(cc_far, None)

        @pl.when(side == core)
        def _():
            returned(1 - cc_far, None)

        @pl.when(side != core)
        def _():
            for h in range(2):
                returned(1 - cc_far, h)

    send_waits()


def store(gate, upper, down, mixed, gate_out, up_out, down_out, mixed_out, sem):
    copies = [
        pltpu.make_async_copy(gate, gate_out.at[0], sem.at[0]),
        pltpu.make_async_copy(upper, up_out.at[0], sem.at[1]),
        pltpu.make_async_copy(down, down_out.at[0], sem.at[2]),
        pltpu.make_async_copy(mixed, mixed_out, sem.at[3]),
    ]
    for c in copies:
        c.start()
    for c in copies:
        c.wait()


def fused(ng, nz, nt, tokens, routes, route_weight, gain, w_gate, w_up, w_down):
    rows, d = tokens.shape
    quarter = d // nt
    experts, chunk, width = w_gate.shape
    chunks = ng * nz
    per_owner = chunks // nt
    cap = 3 * rows // experts
    bf, f32 = jnp.bfloat16, jnp.float32
    dma = pltpu.SemaphoreType.DMA
    full = pltpu.VMEM((d, width), bf)
    vmem = pl.BlockSpec(memory_space=pltpu.VMEM)
    anywhere = pl.BlockSpec(memory_space=pl.ANY)
    results = pl.pallas_call(
        functools.partial(kernel, ng, nz, nt),
        out_shape=(full, full, full, pltpu.VMEM((rows, quarter), bf)),
        in_specs=[anywhere, vmem, vmem, vmem, anywhere, anywhere, anywhere],
        out_specs=(vmem,) * 4,
        scratch_shapes=[
            pltpu.VMEM((nz, rows, d), bf),
            pltpu.VMEM((nz, cap, d), bf),
            pltpu.VMEM((nz, cap, width), bf),
            pltpu.VMEM((chunks, nz, cap, chunk), bf),
            pltpu.VMEM((chunks // 2, nz, cap, chunk), bf),
            pltpu.VMEM((per_owner, nz, cap, chunk), bf),
            pltpu.VMEM((per_owner, nz, rows, chunk), bf),
            pltpu.VMEM((2, nz, chunk, width), bf),
            pltpu.VMEM((rows, d), bf),
            pltpu.VMEM((2, per_owner, rows, chunk), bf),
            pltpu.VMEM((2, per_owner, rows, chunk), bf),
            pltpu.VMEM((nz, 1, rows), f32),
            pltpu.VMEM((nz, 1, rows), f32),
            pltpu.VMEM((nz, cap, 128), f32),
            pltpu.VMEM((chunk, 128), f32),
            pltpu.VMEM((rows, rows), bf),
            pltpu.VMEM((cap, rows), bf),
            pltpu.VMEM((nz, rows, cap), bf),
            dma((4,)),
            dma((2, nz)), dma((nz,)),
            dma((3, nz)), dma((3, nz)),
            dma((nz,)), dma((nz,)),
            dma((2, BLOCKS + 1, nz)), dma((2, BLOCKS + 1, nz)),
            dma((2, BLOCKS + 1, nz)), dma((2, BLOCKS + 1, nz)),
            dma((chunks + 2, nz)), dma((chunks + 2, nz)),
            dma((chunks + 2, nz)), dma((chunks + 2, nz)),
            dma((3, per_owner, 2)), dma((3, per_owner, 2)),
            dma((2, per_owner, 2)), dma((per_owner,)),
        ],
        compiler_params=pltpu.CompilerParams(
            collective_id=0, has_side_effects=True, vmem_limit_bytes=VMEM_LIMIT
        ),
    )(tokens, routes.T, route_weight.T, gain.reshape(1, chunk), w_gate, w_up, w_down)
    whole = jax.ShapeDtypeStruct((1, d, width), bf)
    return pl.pallas_call(
        store,
        out_shape=(whole, whole, whole, jax.ShapeDtypeStruct((rows, quarter), bf)),
        in_specs=[vmem] * 4,
        out_specs=(anywhere,) * 4,
        scratch_shapes=[dma((4,))],
        compiler_params=pltpu.CompilerParams(vmem_limit_bytes=4 * 1024 * 1024),
    )(*results)

EXP_DEV = 1


def body(tokens, routes, route_weight, gain, w_gate, w_up, w_down):
    scaling = gain[None, :, None]
    gate_local = (w_gate * scaling).astype(jnp.bfloat16)
    up_local = (w_up * scaling).astype(jnp.bfloat16)
    gate_mine, up_mine, down_mine = (
        lax.all_to_all(gate_local, "fs", split_axis=0, concat_axis=1, tiled=True),
        lax.all_to_all(up_local, "fs", split_axis=0, concat_axis=1, tiled=True),
        lax.all_to_all(w_down, "fs", split_axis=0, concat_axis=1, tiled=True),
    )
    gate_out, up_out, down_out = (
        lax.all_gather(gate_mine, "gr", axis=1, tiled=True),
        lax.all_gather(up_mine, "gr", axis=1, tiled=True),
        lax.all_gather(down_mine, "gr", axis=1, tiled=True),
    )
    fs_count = lax.axis_size("fs")
    experts = EXP_DEV * fs_count
    tok_rows = tokens.shape[0]
    capacity = 3 * tok_rows // experts
    float_rows = tokens.astype(jnp.float32)
    normed = (
        float_rows * lax.rsqrt(jnp.mean(float_rows * float_rows, axis=-1, keepdims=True) + EPSILON)
    ).astype(jnp.bfloat16)
    flat_ids = routes.reshape(-1)
    onehot = (flat_ids[:, None] == jnp.arange(experts, dtype=jnp.int32)[None, :]).astype(jnp.int32)
    slot_rank = jnp.sum((jnp.cumsum(onehot, axis=0) - onehot) * onehot, axis=-1)
    destination = (flat_ids * capacity + slot_rank).reshape(tok_rows, 2)
    slot_ids = jnp.arange(experts * capacity, dtype=jnp.int32)
    hits = slot_ids[:, None, None] == destination[None, :, :]
    dispatch = jnp.any(hits, axis=-1).astype(jnp.bfloat16)
    outgoing = jnp.dot(dispatch, normed, preferred_element_type=jnp.float32).astype(jnp.bfloat16)
    outgoing = outgoing.reshape(fs_count, EXP_DEV, capacity, tokens.shape[1])
    arrived = lax.all_to_all(outgoing, "fs", split_axis=0, concat_axis=0, tiled=True)
    gate = jnp.einsum("sjnd,jdf->sjnf", arrived, gate_out, preferred_element_type=jnp.float32)
    upper = jnp.einsum("sjnd,jdf->sjnf", arrived, up_out, preferred_element_type=jnp.float32)
    hidden = (jax.nn.silu(gate) * upper).astype(jnp.bfloat16)
    partial_value = jnp.einsum(
        "sjnf,jdf->sjnd", hidden, down_out, preferred_element_type=jnp.float32
    )
    rounded = lax.optimization_barrier(partial_value.astype(jnp.bfloat16))
    summed = lax.psum_scatter(
        rounded.astype(jnp.float32).astype(jnp.bfloat16), "tp", scatter_dimension=3, tiled=True
    )
    back_home = lax.all_to_all(summed, "fs", split_axis=0, concat_axis=0, tiled=True)
    features = back_home.shape[-1]
    flat_back = back_home.reshape(experts * capacity, features).astype(jnp.float32)
    first = jnp.where(slot_ids[None, :] == destination[:, 0:1], route_weight[:, 0:1], 0.0)
    second = jnp.where(slot_ids[None, :] == destination[:, 1:2], route_weight[:, 1:2], 0.0)
    combine_map = first + second
    mixed = jnp.dot(
        combine_map, flat_back, precision=lax.Precision.HIGHEST, preferred_element_type=jnp.float32
    ).astype(jnp.bfloat16)
    return (gate_out, up_out, down_out, mixed)


def solution(mesh):
    in_specs = (
        P(("gr", "fs"), None),
        P(("gr", "fs"), None),
        P(("gr", "fs"), None),
        P(("gr", "fs")),
        P(None, ("gr", "fs"), "tp"),
        P(None, ("gr", "fs"), "tp"),
        P(None, ("gr", "fs"), "tp"),
    )
    out_specs = (
        P("fs", None, "tp"),
        P("fs", None, "tp"),
        P("fs", None, "tp"),
        P(("gr", "fs"), "tp"),
    )
    ng, nz, nt = mesh.shape["gr"], mesh.shape["fs"], mesh.shape["tp"]
    small = ng == 2 and nt == 4 and nz == 4
    work = functools.partial(fused, ng, nz, nt) if small else body
    return jax.shard_map(work, mesh=mesh, in_specs=in_specs, out_specs=out_specs, check_vma=False)
```
